32 devices in a mesh: ep: 8 (over z, y), tp: 4 (over x, core).
Axes of the slice: x: 2, y: 2, z: 4, core: 2. Of those that a mesh axis runs over, the one named last changes fastest.
Arguments:
- tokens: bfloat16 [1024, 2048], P('ep'), may hold values from -6 to 6
- norm_gain: bfloat16 [2048], replicated, may hold values from 0.099609375 to 1.8984375
- expert_ids: int32 [1024, 2], P('ep'), may hold values from 0 to 7, all different within a row; in each aligned block of 128 rows (0 to 127, 128 to 255, ...) at most 48 rows name the same one
- route_weights: float32 [1024, 2], P('ep'), may hold values from 0.2 to 1.5
- gate_weight: bfloat16 [8, 2048, 512], P('ep', None, 'tp'), may hold values from -0.125 to 0.125
- up_weight: bfloat16 [8, 2048, 512], P('ep', None, 'tp'), may hold values from -0.125 to 0.125
- down_weight: bfloat16 [8, 512, 2048], P('ep', 'tp'), may hold values from -0.25 to 0.25
- shared_gate: bfloat16 [2048, 512], P(None, 'tp'), may hold values from -0.125 to 0.125
- shared_up: bfloat16 [2048, 512], P(None, 'tp'), may hold values from -0.125 to 0.125
- shared_down: bfloat16 [512, 2048], P('tp'), may hold values from -0.25 to 0.25
Outputs:
- mixed: bfloat16 [1024, 2048], P('ep', 'tp')
The draws below stay inside these ranges and needn't reach their ends.
Inputs may be any that keep to these rules, and one draw needn't show every extreme that they name: `expert_ids`: each row names 2 different experts. Among the rows of one index of ep (aligned blocks of 128 rows) no expert is named more than 48 times, a bound that some block reaches.
All inputs are finite; a program needn't handle non-finite values.
Results may differ from the reference program's by a relative error of at most 0.012.
Values may be sent and summed in bfloat16 or wider, within the bound.
No kernel may reach another device: no remote copies, remote signals or barrier semaphores. Data moves between devices by JAX's collectives and lax.ppermute only.
A program may use at most 64 MiB of HBM per device.

```python
import math
import jax
import jax.numpy as jnp
import numpy as np
from jax import lax

D = 2048
FF = 512
TOP_K = 2
TOK_GRP = 128
EXPERTS = 8
TOKENS = 1024
CAPACITY = 48
N_EP = 8
N_TP = 4


def shard_levels(own_key, extent, cuts, low, high):
    gain = 1.0
    for axis_at, parts in cuts:
        draws = jax.random.uniform(jax.random.fold_in(jax.random.fold_in(own_key, 6), axis_at), (parts,), jnp.float32, low / len(cuts), high / len(cuts))
        gain = gain * jnp.repeat(jnp.exp(draws), extent[axis_at] // parts).reshape((-1,) + (1,) * (len(extent) - 1 - axis_at))
    return gain


def assign_block(rng, own, number, rows, count, top, bound, lean):
    sequence = jax.random.permutation(rng, count)
    crowded, common = portions_of(count, rows * top, bound, lean, True), portions_of(count, rows * top, bound, lean, False)
    places = jnp.arange(count)

    def named(tallies, offset_by):
        used = int((tallies > 0).sum())
        fixed = max(1, used // 4)
        moved = fixed + (places - fixed + offset_by * (used - fixed)) % max(1, count - fixed)
        return jnp.zeros((count,), jnp.int32).at[sequence[jnp.where(places < fixed, places, moved)]].set(jnp.asarray(tallies, jnp.int32))

    tallies = jnp.where(number % 4 == 0, named(crowded, number // 4), named(common, number - number // 4 - 1))
    mixed = jax.random.permutation(jax.random.fold_in(own, 3), count)
    source_of, sink = mixed[0:count // 2 * 2:2], mixed[1:count // 2 * 2:2]
    room = jnp.minimum(tallies[source_of] - 1, bound - tallies[sink]) // 2
    room = jnp.where((source_of == sequence[0]) | (sink == sequence[0]) | (tallies[sink] == 0), 0, jnp.maximum(room, 0))
    moved = jax.random.randint(jax.random.fold_in(own, 4), (count // 2,), 0, 1 << 20) % (room + 1)
    tallies = tallies.at[source_of].add(-moved).at[sink].add(moved)
    labels = jnp.searchsorted(jnp.cumsum(tallies), jnp.arange(rows * top), side="right").astype(jnp.int32)
    grid = labels.reshape(top, rows).T
    grid = grid[jax.random.permutation(jax.random.fold_in(own, 1), rows)]
    offset_by = jax.random.randint(jax.random.fold_in(own, 2), (rows, 1), 0, top)
    return jnp.take_along_axis(grid, (jnp.arange(top)[None, :] + offset_by) % top, axis=1)


def portions_of(amount, total, reach, slope, full):
    loads = [(1 << 20) // math.isqrt(standing ** slope) + 1 for standing in range(1, amount + 1)]
    largest = reach if full else min(reach, max(-(-total // amount), total * loads[0] // sum(loads)))
    least = 1 if total - largest >= amount - 1 else 0
    given, spare = [largest] + [least] * (amount - 1), total - largest - least * (amount - 1)
    while spare > 0:
        candidates = [i for i in range(1, amount) if given[i] < largest] or [i for i in range(1, amount) if given[i] < reach]
        whole, remaining = sum([loads[i] for i in candidates]), spare
        for i in candidates:
            more = min(reach - given[i], max(1, remaining * loads[i] // whole), spare)
            given[i] = given[i] + more
            spare = spare - more
    return np.array(given)


def centred(key, shape, spread, reach, shards=(), kind=jnp.bfloat16):
    drawn = jax.random.normal(key, shape, jnp.float32) * spread
    if len(shards) > 0:
        drawn = shard_levels(key, shape, shards, -0.22, 0.18) * drawn
    return jnp.clip(drawn, min=-reach, max=reach).astype(kind)


def setup_inputs(seed: int = 0) -> dict:
    splits = jax.random.split(jax.random.key(seed), 11)
    tokens = centred(splits[0], (TOKENS, D), 1.0, 6.0, ((0, 8),))
    norm_gain = jnp.clip(1.0 + 0.18 * jax.random.normal(splits[1], (D,), jnp.float32), 0.099609375, 1.8984375).astype(jnp.bfloat16)
    expert_ids_keys = jax.random.split(jax.random.fold_in(splits[2], 1), TOKENS // TOK_GRP)
    expert_ids_turns = jax.random.permutation(jax.random.fold_in(splits[2], 3), TOKENS // TOK_GRP)
    expert_ids = jax.vmap(lambda own, number: assign_block(jax.random.fold_in(splits[2], 2), own, number, TOK_GRP, EXPERTS, TOP_K, CAPACITY, 2))(expert_ids_keys, expert_ids_turns).reshape((TOKENS, TOP_K))
    route_weights = jnp.clip(0.2 + 1.3 * jax.random.uniform(splits[3], (TOKENS, TOP_K), jnp.float32) ** shard_levels(splits[3], (TOKENS, TOP_K), ((0, 8),), -0.2, 0.2), 0.2, 1.5)
    gate_weight = centred(splits[4], (EXPERTS, D, FF), D ** -0.5, 0.125, ((0, 8), (2, 4)))
    up_weight = centred(splits[5], (EXPERTS, D, FF), D ** -0.5, 0.125, ((0, 8), (2, 4)))
    down_weight = centred(splits[6], (EXPERTS, FF, D), FF ** -0.5, 0.25, ((0, 8), (1, 4)))
    shared_gate = centred(splits[7], (D, FF), D ** -0.5, 0.125, ((1, 4),))
    shared_up = centred(splits[8], (D, FF), D ** -0.5, 0.125, ((1, 4),))
    shared_down = centred(splits[9], (FF, D), FF ** -0.5, 0.25, ((0, 4),))
    return dict(tokens=tokens, norm_gain=norm_gain, expert_ids=expert_ids, route_weights=route_weights, gate_weight=gate_weight, up_weight=up_weight, down_weight=down_weight, shared_gate=shared_gate, shared_up=shared_up, shared_down=shared_down)


norm_eps = 1e-06

def project(rows, w_gate, w_up, w_down):
    gate = jnp.dot(rows, w_gate, preferred_element_type=jnp.float32)
    upper = jnp.dot(rows, w_up, preferred_element_type=jnp.float32)
    hidden = (jax.nn.silu(gate) * upper).astype(jnp.bfloat16)
    block = FF // N_TP
    total = jnp.zeros((rows.shape[0], w_down.shape[1]), jnp.float32)
    for index in range(N_TP):
        piece = jnp.dot(hidden[:, index * block:(index + 1) * block], w_down[index * block:(index + 1) * block], preferred_element_type=jnp.float32).astype(jnp.bfloat16)
        piece = lax.optimization_barrier(piece)
        total = total + piece.astype(jnp.float32)
    return total

def reference(tokens, norm_gain, expert_ids, route_weights, gate_weight, up_weight, down_weight, shared_gate, shared_up, shared_down):
    values = tokens.astype(jnp.float32)
    normed = (values * lax.rsqrt(lax.optimization_barrier(jnp.mean(values * values, axis=-1, keepdims=True)) + norm_eps) * norm_gain.astype(jnp.float32)).astype(jnp.bfloat16)
    shared = project(normed, shared_gate, shared_up, shared_down)
    flat = expert_ids.reshape(-1).astype(jnp.int32)
    pairs = flat.shape[0]
    order = jnp.argsort(flat, stable=True).astype(jnp.int32)
    counts = jnp.bincount(flat, length=EXPERTS).astype(jnp.int32)
    starts = jnp.cumsum(counts) - counts
    sorted_ids = flat[order]
    ranks = jnp.arange(pairs, dtype=jnp.int32) - starts[sorted_ids]
    slots = N_EP * CAPACITY
    table = jnp.full((EXPERTS, slots), pairs, jnp.int32).at[sorted_ids, ranks].set(order)
    padded = jnp.concatenate([normed, jnp.zeros((1, D), jnp.bfloat16)], axis=0)

    def one_expert(expert):
        index = table[expert]
        rows = padded[jnp.minimum(index // TOP_K, TOKENS)]
        return project(rows, gate_weight[expert], up_weight[expert], down_weight[expert]).astype(jnp.bfloat16)
    outputs = lax.map(one_expert, jnp.arange(EXPERTS, dtype=jnp.int32))
    per_pair = jnp.zeros((pairs + 1, D), jnp.bfloat16).at[table.reshape(-1)].set(outputs.reshape(-1, D))
    picked = per_pair[:pairs].reshape(TOKENS, TOP_K, D).astype(jnp.float32)
    total = shared + lax.optimization_barrier(jnp.sum(picked * route_weights[:, :, None], axis=1))
    return total.astype(jnp.bfloat16)
```

```python
import functools

import jax
import jax.numpy as jnp
from jax import lax
from jax.experimental import pallas as pl
from jax.experimental.pallas import tpu as pltpu
from jax.sharding import PartitionSpec as P

norm_eps = 1e-06
f32 = jnp.float32
bf16 = jnp.bfloat16

vmem = pl.BlockSpec(memory_space=pltpu.VMEM)
smem = pl.BlockSpec(memory_space=pltpu.SMEM)


grant = 16 * 1024 * 1024


def call(body, outs, ins, flops, scratch=()):
    moved = sum(a.size * a.dtype.itemsize for a in ins)
    moved += sum(o.size * o.dtype.itemsize for o in outs)
    specs = [smem if a.dtype == jnp.int32 and a.ndim == 1 else vmem for a in ins]
    return pl.pallas_call(
        body,
        out_shape=outs,
        in_specs=specs,
        out_specs=[vmem] * len(outs),
        scratch_shapes=list(scratch),
        compiler_params=pltpu.CompilerParams(vmem_limit_bytes=grant),
        cost_estimate=pl.CostEstimate(flops=flops, bytes_accessed=moved, transcendentals=0),
    )(*ins)


def shape(rows, columns, dtype):
    return jax.ShapeDtypeStruct((rows, columns), dtype)


def route_body(half, mixed, place, ids, gain, tokens, *outs):
    normed_out, slots_out = outs[0], outs[1]
    rows = tokens.shape[0]
    values = tokens[...].astype(f32)
    scale = lax.rsqrt(jnp.mean(values * values, axis=-1, keepdims=True) + norm_eps)
    normed = (values * scale * gain[...].astype(f32)).astype(bf16)
    normed_out[...] = normed
    lanes = max(128, mixed)
    lane = lax.broadcasted_iota(jnp.int32, (rows, lanes), 1)
    before = (
        lax.broadcasted_iota(jnp.int32, (rows, rows), 0)
        > lax.broadcasted_iota(jnp.int32, (rows, rows), 1)
    ).astype(bf16)
    chosen = ids.shape[1]
    base = jnp.zeros((1, lanes), f32)
    total = sum(out.shape[0] for out in outs[2:])
    slot = lax.broadcasted_iota(jnp.int32, (rows, total), 1)
    hit = jnp.zeros((rows, total), jnp.bool_)
    for j in range(chosen):
        expert = ids[:, j : j + 1] ^ place[0]
        onehot = (lane == expert).astype(f32)
        earlier = jnp.dot(before, onehot.astype(bf16), preferred_element_type=f32) + base
        rank = jnp.sum(earlier * onehot, axis=1, keepdims=True).astype(jnp.int32) - place[1]
        base = base + jnp.sum(onehot, axis=0, keepdims=True)
        held = jnp.logical_and(rank >= 0, rank < half)
        where = jnp.where(held, expert * half + rank, -1)
        slots_out[:, j : j + 1] = where
        hit = jnp.logical_or(hit, slot == where)
    pick = hit.astype(f32).T.astype(bf16)
    at = 0
    for out in outs[2:]:
        n = out.shape[0]
        out[...] = jnp.dot(pick[at : at + n], normed, preferred_element_type=f32).astype(bf16)
        at += n


def product_body(blocks, sets, place, *refs):
    rows_in, weights = refs[:blocks], refs[blocks : blocks + 3 * sets]
    send, keep = refs[blocks + 3 * sets : blocks + 3 * sets + 2]
    if blocks > 1:
        gathered = refs[-1]
        at = 0
        for ref in rows_in:
            gathered[at : at + ref.shape[0]] = ref[...]
            at += ref.shape[0]
    else:
        gathered = rows_in[0]
    rows = gathered[...]
    hidden = []
    for s in range(sets):
        gate = jnp.dot(rows, weights[3 * s][...], preferred_element_type=f32)
        up = jnp.dot(rows, weights[3 * s + 1][...], preferred_element_type=f32)
        hidden.append((gate / (1.0 + jnp.exp(-gate)) * up).astype(bf16))
    width = keep.shape[1]
    for out, first in ((send, place[1]), (keep, place[0])):
        columns = pl.ds(pl.multiple_of(first, width), width)
        total = jnp.dot(hidden[0], weights[2][:, columns], preferred_element_type=f32)
        for s in range(1, sets):
            total += jnp.dot(hidden[s], weights[3 * s + 2][:, columns], preferred_element_type=f32)
        out[...] = total.astype(out.dtype)


def products(place, rows, weights, width):
    n = sum(r.shape[0] for r in rows)
    full = rows[0].shape[1]
    hidden = sum(w.shape[1] for w in weights[::3])
    scratch = [pltpu.VMEM((n, full), bf16)] if len(rows) > 1 else []
    return call(
        functools.partial(product_body, len(rows), len(weights) // 3),
        [shape(n, width, bf16), shape(n, width, f32)],
        [place, *rows, *weights],
        6 * n * full * hidden,
        scratch,
    )


def add_body(keep, came, *outs):
    at = 0
    for out in outs:
        n = out.shape[0]
        out[...] = (keep[at : at + n] + came[at : at + n].astype(f32)).astype(bf16)
        at += n


def mix_body(first, blocks, place, slots, gains, *refs):
    rows_in, adds, outs = refs[:blocks], refs[blocks:-3], refs[-3:-1]
    gathered = refs[-1]
    at = 0
    for ref in rows_in:
        gathered[at : at + ref.shape[0]] = ref[...]
        at += ref.shape[0]
    slot = lax.broadcasted_iota(jnp.int32, (slots.shape[0], at), 1) + first
    picks = [(slots[:, j : j + 1] == slot).astype(bf16) for j in range(slots.shape[1])]
    width = outs[0].shape[1]
    for i, out in enumerate(outs):
        columns = pl.ds(pl.multiple_of(place[i], width), width) if len(outs) > 1 else slice(None)
        total = sum(a[:, columns].astype(f32) for a in adds)
        rows = gathered[:, columns]
        for j, pick in enumerate(picks):
            total += gains[:, j : j + 1] * jnp.dot(pick, rows, preferred_element_type=f32)
        out[...] = total


def local(
    tokens,
    norm_gain,
    expert_ids,
    route_weights,
    gate_weight,
    up_weight,
    down_weight,
    shared_gate,
    shared_up,
    shared_down,
):
    rows_here, width = tokens.shape
    chosen = expert_ids.shape[1]
    groups = lax.axis_size("ep")
    cuts = lax.axis_size("tp")
    local_experts = gate_weight.shape[0]
    assert local_experts == 1 and cuts == 4
    experts_all = groups * local_experts
    capacity = (3 * rows_here * chosen + 2 * experts_all - 1) // (2 * experts_all)
    half = -(-capacity // 2)
    wide, share = width // 2, width // 4
    direct = groups <= 8
    me, across = lax.axis_index("ep"), lax.axis_index("tp")
    core, side = across % 2, across // 2
    sibling = [(i, i ^ 1) for i in range(cuts)]
    neighbour = [(i, i ^ 2) for i in range(cuts)]
    own = (gate_weight[0], up_weight[0], down_weight[0])
    other = tuple(lax.ppermute(w, "tp", sibling) for w in own)

    if direct:
        sizes = [half] * groups
    else:
        sizes = [half * groups]
    place = jnp.stack([me if direct else jnp.zeros_like(me), core * half]).astype(jnp.int32)
    normed, slots, *sends = call(
        functools.partial(route_body, half, experts_all),
        [shape(rows_here, width, bf16), shape(rows_here, chosen, jnp.int32)]
        + [shape(n, width, bf16) for n in sizes],
        [place, expert_ids, norm_gain.reshape(1, width), tokens],
        2 * rows_here * width * sum(sizes),
    )

    def exchange(blocks, names):
        if not direct:
            return [lax.all_to_all(b, "ep", split_axis=0, concat_axis=0, tiled=True) for b in blocks]
        return [
            b if k == 0 else lax.ppermute(b, "ep", [(i, i ^ k) for i in range(groups)])
            for b, k in zip(blocks, names)
        ]

    blocks = list(range(len(sizes)))
    cut = len(blocks) // 2
    parties = [blocks[cut:], blocks[:cut]] if direct else [blocks]
    arrived = [exchange([sends[k] for k in party], party) for party in parties]

    columns = jnp.stack([side * wide, (1 - side) * wide]).astype(jnp.int32)
    sh_send, sh_keep = products(
        columns, [normed], [shared_gate, shared_up, shared_down], wide
    )
    sh_came = lax.ppermute(sh_send, "tp", neighbour)

    returned = [None] * len(parties)
    for p in reversed(range(len(parties))):
        send, keep = products(columns, arrived[p], [*own, *other], wide)
        came = lax.ppermute(send, "tp", neighbour)
        outs = call(
            add_body,
            [shape(sizes[k], wide, bf16) for k in parties[p]],
            [keep, came],
            keep.size,
        )
        returned[p] = exchange(outs, parties[p])

    ends = jnp.stack([core * share, (1 - core) * share]).astype(jnp.int32)
    rows = [b for p in reversed(range(len(parties))) for b in returned[p]]
    kept, sent = call(
        functools.partial(mix_body, 0, len(rows)),
        [shape(rows_here, share, f32), shape(rows_here, share, f32)],
        [ends, slots, route_weights, *rows, sh_keep, sh_came],
        4 * rows_here * wide * half * groups,
        [pltpu.VMEM((half * groups, wide), bf16)],
    )
    return (kept + lax.ppermute(sent, "tp", sibling)).astype(bf16)


def solution(mesh):
    in_specs = (
        P("ep", None),
        P(),
        P("ep", None),
        P("ep", None),
        P("ep", None, "tp"),
        P("ep", None, "tp"),
        P("ep", "tp", None),
        P(None, "tp"),
        P(None, "tp"),
        P("tp", None),
    )
    out_specs = P("ep", "tp")
    return jax.shard_map(local, mesh=mesh, in_specs=in_specs, out_specs=out_specs, check_vma=False)
```

```python
import functools

import jax
import jax.numpy as jnp
from jax import lax
from jax.experimental import pallas as pl
from jax.experimental.pallas import tpu as pltpu
from jax.sharding import PartitionSpec as P

norm_eps = 1e-06
grant = 16 * 1024 * 1024
f32 = jnp.float32
bf16 = jnp.bfloat16

vmem = pl.BlockSpec(memory_space=pltpu.VMEM)


def call(body, outs, ins, flops, scratch=()):
    moved = sum(a.size * a.dtype.itemsize for a in ins)
    moved += sum(o.size * o.dtype.itemsize for o in outs)
    return pl.pallas_call(
        body,
        out_shape=outs,
        in_specs=[vmem] * len(ins),
        out_specs=[vmem] * len(outs),
        scratch_shapes=list(scratch),
        compiler_params=pltpu.CompilerParams(vmem_limit_bytes=grant),
        cost_estimate=pl.CostEstimate(flops=flops, bytes_accessed=moved, transcendentals=0),
    )(*ins)


def shape(rows, columns, dtype):
    return jax.ShapeDtypeStruct((rows, columns), dtype)


def route_body(half, experts, relabel, ids, gain, tokens, *outs):
    normed_out, slots_out = outs[0], outs[1]
    rows, width = tokens.shape
    values = tokens[...].astype(f32)
    scale = lax.rsqrt(jnp.mean(values * values, axis=-1, keepdims=True) + norm_eps)
    lanes = gain.shape[1]
    for c in range(width // lanes):
        at = slice(c * lanes, (c + 1) * lanes)
        normed_out[:, at] = (values[:, at] * scale * gain[c : c + 1].astype(f32)).astype(bf16)
    mixed = lax.axis_index("ep") if relabel else 0
    first = (lax.axis_index("tp") % 2) * half
    kinds = max(8, experts)
    kind = lax.broadcasted_iota(jnp.int32, (kinds, rows), 0)
    before = (
        lax.broadcasted_iota(jnp.int32, (rows, rows), 0)
        < lax.broadcasted_iota(jnp.int32, (rows, rows), 1)
    ).astype(bf16)
    base = jnp.zeros((kinds, 1), f32)
    total = sum(out.shape[0] for out in outs[2:])
    slot = lax.broadcasted_iota(jnp.int32, (total, rows), 0)
    hit = jnp.zeros((total, rows), f32)
    for j in range(ids.shape[0]):
        expert = ids[j : j + 1, :] ^ mixed
        onehot = (kind == expert).astype(f32)
        earlier = jnp.dot(onehot.astype(bf16), before, preferred_element_type=f32) + base
        rank = jnp.sum(earlier * onehot, axis=0, keepdims=True).astype(jnp.int32) - first
        base = base + jnp.sum(onehot, axis=1, keepdims=True)
        held = jnp.logical_and(rank >= 0, rank < half)
        where = jnp.where(held, expert * half + rank, -1)
        slots_out[j : j + 1, :] = where
        hit = jnp.where(slot == where, 1.0, hit)
    pick = hit.astype(bf16)
    normed = normed_out[...]
    at = 0
    for out in outs[2:]:
        n = out.shape[0]
        out[...] = jnp.dot(pick[at : at + n], normed, preferred_element_type=f32).astype(bf16)
        at += n


def product_body(blocks, sets, *refs):
    rows_in, weights = refs[:blocks], refs[blocks : blocks + 3 * sets]
    send, keep = refs[blocks + 3 * sets : blocks + 3 * sets + 2]
    if blocks > 1:
        gathered = refs[-1]
        at = 0
        for ref in rows_in:
            gathered[at : at + ref.shape[0]] = ref[...]
            at += ref.shape[0]
    else:
        gathered = rows_in[0]
    side = lax.axis_index("tp") // 2
    into = [w[...] for w in weights[::3]] + [w[...] for w in weights[1::3]]
    both = jnp.dot(gathered[...], jnp.concatenate(into, axis=1), preferred_element_type=f32)
    units = both.shape[1] // 2
    gate, up = both[:, :units], both[:, units:]
    hidden = (gate / (1.0 + jnp.exp(-gate)) * up).astype(bf16)
    width = keep.shape[1]
    for out, place in ((send, 1 - side), (keep, side)):
        columns = pl.ds(pl.multiple_of(place * width, width), width)
        down = jnp.concatenate([w[:, columns] for w in weights[2::3]], axis=0)
        out[...] = jnp.dot(hidden, down, preferred_element_type=f32).astype(out.dtype)


def products(rows, weights, width):
    n = sum(r.shape[0] for r in rows)
    full = rows[0].shape[1]
    hidden = sum(w.shape[1] for w in weights[::3])
    scratch = [pltpu.VMEM((n, full), bf16)] if len(rows) > 1 else []
    return call(
        functools.partial(product_body, len(rows), len(weights) // 3),
        [shape(n, width, bf16), shape(n, width, f32)],
        [*rows, *weights],
        6 * n * full * hidden,
        scratch,
    )


def add_body(keep, came, *outs):
    at = 0
    for out in outs:
        n = out.shape[0]
        out[...] = (keep[at : at + n] + came[at : at + n].astype(f32)).astype(out.dtype)
        at += n


def mix_body(blocks, slots, gains, *refs):
    rows_in, adds, outs = refs[:blocks], refs[blocks:-3], refs[-3:-1]
    gathered = refs[-1]
    at = 0
    for ref in rows_in:
        gathered[at : at + ref.shape[0]] = ref[...]
        at += ref.shape[0]
    tokens = slots.shape[1]
    slot = lax.broadcasted_iota(jnp.int32, (at, tokens), 0)
    weight = jnp.zeros((at, tokens), f32)
    for j in range(slots.shape[0]):
        weight = jnp.where(slot == slots[j : j + 1, :], gains[j : j + 1, :], weight)
    weight = weight.T
    high = weight.astype(bf16)
    low = (weight - high.astype(f32)).astype(bf16)
    width = outs[0].shape[1]
    core = lax.axis_index("tp") % 2
    for out, place in ((outs[0], core), (outs[1], 1 - core)):
        columns = pl.ds(pl.multiple_of(place * width, width), width)
        rows = gathered[:, columns]
        total = sum(a[:, columns].astype(f32) for a in adds)
        total += jnp.dot(high, rows, preferred_element_type=f32)
        out[...] = total + jnp.dot(low, rows, preferred_element_type=f32)


def local(
    tokens,
    norm_gain,
    expert_ids,
    route_weights,
    gate_weight,
    up_weight,
    down_weight,
    shared_gate,
    shared_up,
    shared_down,
):
    rows_here, width = tokens.shape
    chosen = expert_ids.shape[1]
    groups = lax.axis_size("ep")
    cuts = lax.axis_size("tp")
    local_experts = gate_weight.shape[0]
    assert local_experts == 1 and cuts == 4
    capacity = (3 * rows_here * chosen + 2 * groups - 1) // (2 * groups)
    half = -(-capacity // 2)
    wide, share = width // 2, width // 4
    direct = groups == 8
    sibling = [(i, i ^ 1) for i in range(cuts)]
    neighbour = [(i, i ^ 2) for i in range(cuts)]
    own = (gate_weight[0], up_weight[0], down_weight[0])
    other = tuple(lax.ppermute(w, "tp", sibling) for w in own)

    sizes = [half] * groups if direct else [half * groups]
    normed, slots, *sends = call(
        functools.partial(route_body, half, groups, direct),
        [shape(rows_here, width, bf16), shape(chosen, rows_here, jnp.int32)]
        + [shape(n, width, bf16) for n in sizes],
        [expert_ids.T, norm_gain.reshape(-1, 128), tokens],
        2 * rows_here * width * sum(sizes),
    )

    def exchange(k, block):
        if not direct:
            return lax.all_to_all(block, "ep", split_axis=0, concat_axis=0, tiled=True)
        if k == 0:
            return block
        return lax.ppermute(block, "ep", [(i, i ^ k) for i in range(groups)])

    parties = {"A": [4, 5], "N": [0, 1, 2, 3], "B": [6, 7]} if direct else {"A": [0]}
    arrived = [exchange(k, sends[k]) for k in range(len(sizes))]
    sh_send, sh_keep = products([normed], [shared_gate, shared_up, shared_down], wide)
    sh_came = lax.ppermute(sh_send, "tp", neighbour)

    returned = [None] * len(sizes)
    for names in parties.values():
        send, keep = products([arrived[k] for k in names], [*own, *other], wide)
        came = lax.ppermute(send, "tp", neighbour)
        outs = call(add_body, [shape(sizes[k], wide, bf16) for k in names], [keep, came], keep.size)
        for k, out in zip(names, outs):
            returned[k] = exchange(k, out)

    kept, sent = call(
        functools.partial(mix_body, len(returned)),
        [shape(rows_here, share, f32), shape(rows_here, share, f32)],
        [slots, route_weights.T, *returned, sh_keep, sh_came],
        4 * rows_here * wide * half * groups,
        [pltpu.VMEM((half * groups, wide), bf16)],
    )
    came = lax.ppermute(sent, "tp", sibling)
    (mixed,) = call(add_body, [shape(rows_here, share, bf16)], [kept, came], kept.size)
    return mixed


def solution(mesh):
    in_specs = (
        P("ep", None),
        P(),
        P("ep", None),
        P("ep", None),
        P("ep", None, "tp"),
        P("ep", None, "tp"),
        P("ep", "tp", None),
        P(None, "tp"),
        P(None, "tp"),
        P("tp", None),
    )
    out_specs = P("ep", "tp")

    return jax.shard_map(local, mesh=mesh, in_specs=in_specs, out_specs=out_specs, check_vma=False)
```

```python
import functools

import jax
import jax.numpy as jnp
from jax import lax
from jax.experimental import pallas as pl
from jax.experimental.pallas import tpu as pltpu
from jax.sharding import PartitionSpec as P

norm_eps = 1e-06
grant = 16 * 1024 * 1024
f32 = jnp.float32
bf16 = jnp.bfloat16

vmem = pl.BlockSpec(memory_space=pltpu.VMEM)
hbm = pl.BlockSpec(memory_space=pltpu.HBM)


def call(body, outs, ins, flops, scratch=(), far=()):
    moved = sum(a.size * a.dtype.itemsize for a in ins)
    moved += sum(o.size * o.dtype.itemsize for o in outs)
    ins = [
        pltpu.with_memory_space_constraint(a, pltpu.HBM) if i in far else a for i, a in enumerate(ins)
    ]
    return pl.pallas_call(
        body,
        out_shape=outs,
        in_specs=[hbm if i in far else vmem for i in range(len(ins))],
        out_specs=[vmem] * len(outs),
        scratch_shapes=list(scratch),
        compiler_params=pltpu.CompilerParams(vmem_limit_bytes=grant),
        cost_estimate=pl.CostEstimate(flops=flops, bytes_accessed=moved, transcendentals=0),
    )(*ins)


def landing(arrays):
    return [pltpu.VMEM(a.shape, a.dtype) for a in arrays] + [pltpu.SemaphoreType.DMA((len(arrays),))]


def fetch(sources, targets, sems):
    copies = [
        pltpu.make_async_copy(s, t, sems.at[i]) for i, (s, t) in enumerate(zip(sources, targets))
    ]
    for copy in copies:
        copy.start()
    return copies


def shape(rows, columns, dtype):
    return jax.ShapeDtypeStruct((rows, columns), dtype)


def route_body(half, experts, far, kept, ids_in, gain_in, tokens_in, *refs):
    outs, (ids, gain, tokens, sems) = refs[:-4], refs[-4:]
    copies = fetch((ids_in, gain_in, tokens_in), (ids, gain, tokens), sems)
    normed_out, slots_out = outs[0], outs[1]
    rows, width = tokens.shape
    mixed = lax.axis_index("ep") if far else 0
    side = lax.axis_index("tp") // 2
    first = (lax.axis_index("tp") % 2) * half
    kinds = max(8, experts)
    kind = lax.broadcasted_iota(jnp.int32, (kinds, rows), 0)
    before = (
        lax.broadcasted_iota(jnp.int32, (rows, rows), 0)
        < lax.broadcasted_iota(jnp.int32, (rows, rows), 1)
    ).astype(bf16)
    base = jnp.zeros((kinds, 1), f32)
    total = experts * half
    slot = lax.broadcasted_iota(jnp.int32, (total, rows), 0)
    hit = jnp.zeros((total, rows), f32)
    copies[0].wait()
    for j in range(ids.shape[0]):
        label = ids[j : j + 1, :] ^ mixed
        if far:
            label = jnp.where(label >= far, label ^ side, label)
        onehot = (kind == label).astype(f32)
        earlier = jnp.dot(onehot.astype(bf16), before, preferred_element_type=f32) + base
        rank = jnp.sum(earlier * onehot, axis=0, keepdims=True).astype(jnp.int32) - first
        base = base + jnp.sum(onehot, axis=1, keepdims=True)
        held = jnp.logical_and(rank >= 0, rank < half)
        where = jnp.where(held, label * half + rank, -1)
        slots_out[j : j + 1, :] = where
        hit = jnp.where(slot == where, 1.0, hit)
    pick = hit.astype(bf16)
    copies[1].wait()
    copies[2].wait()
    values = tokens[...].astype(f32)
    scale = lax.rsqrt(jnp.mean(values * values, axis=-1, keepdims=True) + norm_eps)
    lanes = gain.shape[1]
    for c in range(width // lanes):
        at = slice(c * lanes, (c + 1) * lanes)
        normed_out[:, at] = (values[:, at] * scale * gain[c : c + 1].astype(f32)).astype(bf16)
    normed = normed_out[...]
    for k, out in zip(kept, outs[2:]):
        n = out.shape[0]
        part = pick[k * n : (k + 1) * n]
        out[...] = jnp.dot(part, normed, preferred_element_type=f32).astype(bf16)


def product_body(blocks, sets, swap, fetched, *refs):
    rows_in, weights = refs[:blocks], refs[blocks : blocks + 3 * sets]
    send, keep = refs[blocks + 3 * sets : blocks + 3 * sets + 2]
    rest = refs[blocks + 3 * sets + 2 :]
    if fetched:
        copies = fetch(weights, rest[:-1], rest[-1])
        weights = rest[:-1]
    if blocks > 1:
        gathered = rest[0]
        at = 0
        for ref in rows_in:
            gathered[at : at + ref.shape[0]] = ref[...]
            at += ref.shape[0]
    else:
        gathered = rows_in[0]
    side = lax.axis_index("tp") // 2
    if fetched:
        for copy in copies:
            copy.wait()
    into = [w[...] for w in weights[::3]] + [w[...] for w in weights[1::3]]
    both = jnp.dot(gathered[...], jnp.concatenate(into, axis=1), preferred_element_type=f32)
    units = both.shape[1] // 2
    gate, up = both[:, :units], both[:, units:]
    hidden = (gate / (1.0 + jnp.exp(-gate)) * up).astype(bf16)
    width = keep.shape[1]
    step = rows_in[0].shape[0]
    for out, place in ((send, 1 - side), (keep, side)):
        columns = pl.ds(pl.multiple_of(place * width, width), width)
        down = jnp.concatenate([w[:, columns] for w in weights[2::3]], axis=0)
        total = jnp.dot(hidden, down, preferred_element_type=f32).astype(out.dtype)
        if out is send and blocks > 1:
            for b in range(blocks):
                c = b ^ 1 if swap[b] else b
                out[c * step : (c + 1) * step] = total[b * step : (b + 1) * step]
        else:
            out[...] = total


def products(rows, weights, width, swap=(), fetched=False):
    n = sum(r.shape[0] for r in rows)
    full = rows[0].shape[1]
    hidden = sum(w.shape[1] for w in weights[::3])
    scratch = [pltpu.VMEM((n, full), bf16)] if len(rows) > 1 else []
    far = ()
    if fetched:
        scratch = landing(weights)
        far = range(len(rows), len(rows) + len(weights))
    return call(
        functools.partial(product_body, len(rows), len(weights) // 3, swap, fetched),
        [shape(n, width, bf16), shape(n, width, f32)],
        [*rows, *weights],
        6 * n * full * hidden,
        scratch,
        far,
    )


def add_body(keep, came, *outs):
    at = 0
    for out in outs:
        n = out.shape[0]
        out[...] = (keep[at : at + n] + came[at : at + n].astype(f32)).astype(out.dtype)
        at += n


def plan_body(slots, gains_in, high_out, low_out, gains, sems):
    (copy,) = fetch((gains_in,), (gains,), sems)
    slot = lax.broadcasted_iota(jnp.int32, high_out.shape[::-1], 0)
    weight = jnp.zeros(slot.shape, f32)
    copy.wait()
    for j in range(slots.shape[0]):
        weight = jnp.where(slot == slots[j : j + 1, :], gains[j : j + 1, :], weight)
    weight = weight.T
    high = weight.astype(bf16)
    high_out[...] = high
    low_out[...] = (weight - high.astype(f32)).astype(bf16)


def mix_body(blocks, high, low, *refs):
    rows_in, adds, outs = refs[:blocks], refs[blocks:-3], refs[-3:-1]
    gathered = refs[-1]
    at = 0
    for ref in rows_in:
        gathered[at : at + ref.shape[0]] = ref[...]
        at += ref.shape[0]
    width = outs[0].shape[1]
    core = lax.axis_index("tp") % 2
    for out, place in ((outs[0], core), (outs[1], 1 - core)):
        columns = pl.ds(pl.multiple_of(place * width, width), width)
        rows = gathered[:, columns]
        total = sum(a[:, columns].astype(f32) for a in adds)
        total += jnp.dot(high[...], rows, preferred_element_type=f32)
        out[...] = total + jnp.dot(low[...], rows, preferred_element_type=f32)


def local(
    tokens,
    norm_gain,
    expert_ids,
    route_weights,
    gate_weight,
    up_weight,
    down_weight,
    shared_gate,
    shared_up,
    shared_down,
):
    rows_here, width = tokens.shape
    chosen = expert_ids.shape[1]
    groups = lax.axis_size("ep")
    cuts = lax.axis_size("tp")
    local_experts = gate_weight.shape[0]
    assert local_experts == 1 and cuts == 4
    capacity = (3 * rows_here * chosen + 2 * groups - 1) // (2 * groups)
    half = -(-capacity // 2)
    wide, share = width // 2, width // 4
    direct = groups == 8
    far = groups // 2 if direct else 0
    sibling = [(i, i ^ 1) for i in range(cuts)]
    neighbour = [(i, i ^ 2) for i in range(cuts)]
    own = (gate_weight[0], up_weight[0], down_weight[0])
    other = tuple(lax.ppermute(w, "tp", sibling) for w in own)

    def hop(k, block):
        if not direct:
            return lax.all_to_all(block, "ep", split_axis=0, concat_axis=0, tiled=True)
        if k == 0:
            return block
        pairs = []
        for i in range(groups):
            for t in range(cuts):
                to = i ^ (k ^ (t // 2) if k >= far else k)
                pairs.append((i * cuts + t, to * cuts + t))
        return lax.ppermute(block, ("ep", "tp"), pairs)

    sizes = [half] * groups if direct else [half * groups]
    kept = [0, 1, 2, 3, 4, 7] if direct else [0]
    args = [expert_ids.T, norm_gain.reshape(-1, 128), tokens]
    normed, slots, *sends = call(
        functools.partial(route_body, half, groups, far, kept),
        [shape(rows_here, width, bf16), shape(chosen, rows_here, jnp.int32)]
        + [shape(sizes[k], width, bf16) for k in kept],
        args,
        2 * rows_here * width * half * groups,
        landing(args),
        range(3),
    )
    arrived = {k: hop(k, block) for k, block in zip(kept, sends)}
    if direct:
        arrived[5] = lax.ppermute(arrived[4], "tp", neighbour)
        arrived[6] = lax.ppermute(arrived[7], "tp", neighbour)
    sh_send, sh_keep = products([normed], [shared_gate, shared_up, shared_down], wide, fetched=True)
    sh_came = lax.ppermute(sh_send, "tp", neighbour)
    gains = route_weights.T
    high, low = call(
        plan_body,
        [shape(rows_here, half * groups, bf16)] * 2,
        [slots, gains],
        rows_here * half * groups,
        landing([gains]),
        [1],
    )

    returned = [None] * len(sizes)
    for names in (parties if direct else {"A": [0]}).values():
        swap = [far > 0 and k >= far for k in names]
        send, keep = products([arrived[k] for k in names], [*own, *other], wide, swap)
        came = lax.ppermute(send, "tp", neighbour)
        outs = call(add_body, [shape(sizes[k], wide, bf16) for k in names], [keep, came], keep.size)
        for k, out in zip(names, outs):
            returned[k] = hop(k, out)

    mine, sent = call(
        functools.partial(mix_body, len(returned)),
        [shape(rows_here, share, f32), shape(rows_here, share, f32)],
        [high, low, *returned, sh_keep, sh_came],
        4 * rows_here * wide * half * groups,
        [pltpu.VMEM((half * groups, wide), bf16)],
    )
    came = lax.ppermute(sent, "tp", sibling)
    (mixed,) = call(add_body, [shape(rows_here, share, bf16)], [mine, came], mine.size)
    return mixed


parties = {"N": [0, 1, 2, 3], "A": [4, 5], "B": [6, 7]}


def solution(mesh):
    in_specs = (
        P("ep", None),
        P(),
        P("ep", None),
        P("ep", None),
        P("ep", None, "tp"),
        P("ep", None, "tp"),
        P("ep", "tp", None),
        P(None, "tp"),
        P(None, "tp"),
        P("tp", None),
    )
    out_specs = P("ep", "tp")

    return jax.shard_map(local, mesh=mesh, in_specs=in_specs, out_specs=out_specs, check_vma=False)
```

```python
import functools

import jax
import jax.numpy as jnp
from jax import lax
from jax.experimental import pallas as pl
from jax.experimental.pallas import tpu as pltpu
from jax.sharding import PartitionSpec as P

norm_eps = 1e-06
grant = 16 * 1024 * 1024
f32 = jnp.float32
bf16 = jnp.bfloat16

vmem = pl.BlockSpec(memory_space=pltpu.VMEM)
hbm = pl.BlockSpec(memory_space=pltpu.HBM)


def call(body, outs, ins, flops, scratch=(), far=()):
    moved = sum(a.size * a.dtype.itemsize for a in ins)
    moved += sum(o.size * o.dtype.itemsize for o in outs)
    ins = [
        pltpu.with_memory_space_constraint(a, pltpu.HBM) if i in far else a for i, a in enumerate(ins)
    ]
    return pl.pallas_call(
        body,
        out_shape=outs,
        in_specs=[hbm if i in far else vmem for i in range(len(ins))],
        out_specs=[vmem] * len(outs),
        scratch_shapes=list(scratch),
        compiler_params=pltpu.CompilerParams(vmem_limit_bytes=grant),
        cost_estimate=pl.CostEstimate(flops=flops, bytes_accessed=moved, transcendentals=0),
    )(*ins)


def landing(arrays):
    return [pltpu.VMEM(a.shape, a.dtype) for a in arrays] + [pltpu.SemaphoreType.DMA((len(arrays),))]


def fetch(sources, targets, sems):
    copies = [
        pltpu.make_async_copy(s, t, sems.at[i]) for i, (s, t) in enumerate(zip(sources, targets))
    ]
    for copy in copies:
        copy.start()
    return copies


def shape(rows, columns, dtype):
    return jax.ShapeDtypeStruct((rows, columns), dtype)


def slot_of(label, rank, capacity, direct):
    core, side = lax.axis_index("tp") % 2, lax.axis_index("tp") // 2
    if direct:
        near = label < 4
        holder = jnp.where(near, (label ^ (label >> 1)) & 1, (label >> 1) & 1)
        first = jnp.where((label ^ side) == 4 + 3 * core, 2, 3)
        block = jnp.where(near, label >> 1, first)
        return jnp.where(holder == core, block * capacity + rank, -1)
    half = -(-capacity // 2)
    rank = rank - core * half
    held = jnp.logical_and(rank >= 0, rank < half)
    return jnp.where(held, label * half + rank, -1)


def route_body(capacity, experts, direct, ids_in, gain_in, tokens_in, *refs):
    outs, (ids, gain, tokens, sems) = refs[:-4], refs[-4:]
    copies = fetch((ids_in, gain_in, tokens_in), (ids, gain, tokens), sems)
    normed_out, slots_out = outs[0], outs[1]
    rows, width = tokens.shape
    kinds = max(8, experts)
    kind = lax.broadcasted_iota(jnp.int32, (kinds, rows), 0)
    before = (
        lax.broadcasted_iota(jnp.int32, (rows, rows), 0)
        < lax.broadcasted_iota(jnp.int32, (rows, rows), 1)
    ).astype(bf16)
    base = jnp.zeros((kinds, 1), f32)
    total = sum(out.shape[0] for out in outs[2:])
    slot = lax.broadcasted_iota(jnp.int32, (total, rows), 0)
    hit = jnp.zeros((total, rows), f32)
    copies[0].wait()
    for j in range(ids.shape[0]):
        label = ids[j : j + 1, :]
        if direct:
            label = label ^ lax.axis_index("ep")
        onehot = (kind == label).astype(f32)
        earlier = jnp.dot(onehot.astype(bf16), before, preferred_element_type=f32) + base
        rank = jnp.sum(earlier * onehot, axis=0, keepdims=True).astype(jnp.int32)
        base = base + jnp.sum(onehot, axis=1, keepdims=True)
        where = slot_of(label, rank, capacity, direct)
        slots_out[j : j + 1, :] = where
        hit = jnp.where(slot == where, 1.0, hit)
    pick = hit.astype(bf16)
    copies[1].wait()
    copies[2].wait()
    values = tokens[...].astype(f32)
    scale = lax.rsqrt(jnp.mean(values * values, axis=-1, keepdims=True) + norm_eps)
    lanes = gain.shape[1]
    for c in range(width // lanes):
        at = slice(c * lanes, (c + 1) * lanes)
        normed_out[:, at] = (values[:, at] * scale * gain[c : c + 1].astype(f32)).astype(bf16)
    normed = normed_out[...]
    at = 0
    for out in outs[2:]:
        n = out.shape[0]
        part = pick[at : at + n]
        out[...] = jnp.dot(part, normed, preferred_element_type=f32).astype(bf16)
        at += n


def units_of(rows, weights):
    into = [w[...] for w in weights[::3]] + [w[...] for w in weights[1::3]]
    both = jnp.dot(rows, jnp.concatenate(into, axis=1), preferred_element_type=f32)
    units = both.shape[1] // 2
    gate, up = both[:, :units], both[:, units:]
    return (gate / (1.0 + jnp.exp(-gate)) * up).astype(bf16)


def shared_body(slots, rows, gains_in, *refs):
    weights_in, (send, keep, high_out, low_out) = refs[:3], refs[3:7]
    gains, weights, sems = refs[7], refs[8:11], refs[11]
    copies = fetch((gains_in, *weights_in), (gains, *weights), sems)
    slot = lax.broadcasted_iota(jnp.int32, high_out.shape[::-1], 0)
    weight = jnp.zeros(slot.shape, f32)
    copies[0].wait()
    for j in range(slots.shape[0]):
        weight = jnp.where(slot == slots[j : j + 1, :], gains[j : j + 1, :], weight)
    weight = weight.T
    high = weight.astype(bf16)
    high_out[...] = high
    low_out[...] = (weight - high.astype(f32)).astype(bf16)
    for copy in copies[1:]:
        copy.wait()
    columns_out(units_of(rows[...], weights), weights, send, keep)


def columns_out(hidden, weights, send, keep):
    side = lax.axis_index("tp") // 2
    width = keep.shape[1]
    for out, place in ((send, 1 - side), (keep, side)):
        columns = pl.ds(pl.multiple_of(place * width, width), width)
        down = jnp.concatenate([w[:, columns] for w in weights[2::3]], axis=0)
        out[...] = jnp.dot(hidden, down, preferred_element_type=f32).astype(out.dtype)


def product_body(blocks, *refs):
    rows_in, weights = refs[:blocks], refs[blocks : blocks + 6]
    send, keep = refs[blocks + 6 : blocks + 8]
    gathered = rows_in[0]
    if blocks > 1:
        gathered = refs[-1]
        at = 0
        for ref in rows_in:
            gathered[at : at + ref.shape[0]] = ref[...]
            at += ref.shape[0]
    columns_out(units_of(gathered[...], weights), weights, send, keep)


def products(rows, weights, width):
    n = sum(r.shape[0] for r in rows)
    full = rows[0].shape[1]
    hidden = sum(w.shape[1] for w in weights[::3])
    return call(
        functools.partial(product_body, len(rows)),
        [shape(n, width, bf16), shape(n, width, f32)],
        [*rows, *weights],
        6 * n * full * hidden,
        [pltpu.VMEM((n, full), bf16)] if len(rows) > 1 else [],
    )


def add_body(keep, came, *outs):
    at = 0
    for out in outs:
        n = out.shape[0]
        out[...] = (keep[at : at + n] + came[at : at + n].astype(f32)).astype(out.dtype)
        at += n


def mix_body(blocks, high, low, *refs):
    rows_in, adds, outs = refs[:blocks], refs[blocks:-3], refs[-3:-1]
    gathered = refs[-1]
    at = 0
    for ref in rows_in:
        gathered[at : at + ref.shape[0]] = ref[...]
        at += ref.shape[0]
    width = outs[0].shape[1]
    core = lax.axis_index("tp") % 2
    for out, place in ((outs[0], core), (outs[1], 1 - core)):
        columns = pl.ds(pl.multiple_of(place * width, width), width)
        rows = gathered[:, columns]
        total = sum(a[:, columns].astype(f32) for a in adds)
        total += jnp.dot(high[...], rows, preferred_element_type=f32)
        out[...] = total + jnp.dot(low[...], rows, preferred_element_type=f32)


def local(
    tokens,
    norm_gain,
    expert_ids,
    route_weights,
    gate_weight,
    up_weight,
    down_weight,
    shared_gate,
    shared_up,
    shared_down,
):
    rows_here, width = tokens.shape
    chosen = expert_ids.shape[1]
    groups = lax.axis_size("ep")
    cuts = lax.axis_size("tp")
    local_experts = gate_weight.shape[0]
    assert local_experts == 1 and cuts == 4
    capacity = (3 * rows_here * chosen + 2 * groups - 1) // (2 * groups)
    wide, share = width // 2, width // 4
    direct = groups == 8
    sibling = [(i, i ^ 1) for i in range(cuts)]
    neighbour = [(i, i ^ 2) for i in range(cuts)]
    own = (gate_weight[0], up_weight[0], down_weight[0])
    other = tuple(lax.ppermute(w, "tp", sibling) for w in own)

    def hop(block, between):
        if not direct:
            return lax.all_to_all(block, "ep", split_axis=0, concat_axis=0, tiled=True)
        pairs = []
        for i in range(groups):
            for t in range(cuts):
                pairs.append((i * cuts + t, (i ^ between(t // 2, t % 2)) * cuts + t))
        return lax.ppermute(block, ("ep", "tp"), pairs)

    distances = {
        "P": lambda x, c: c,
        "Q": lambda x, c: 3 - c,
        "A": lambda x, c: (4 + 3 * c) ^ x,
        "B": lambda x, c: (4 + 3 * c) ^ x ^ 1,
    }
    half = -(-capacity // 2)
    sizes = {k: capacity for k in distances} if direct else {"P": half * groups}
    sent_here = [k for k in sizes if k != "B"]
    total = sum(sizes.values())
    args = [expert_ids.T, norm_gain.reshape(-1, 128), tokens]
    normed, slots, *sends = call(
        functools.partial(route_body, capacity, groups, direct),
        [shape(rows_here, width, bf16), shape(chosen, rows_here, jnp.int32)]
        + [shape(sizes[k], width, bf16) for k in sent_here],
        args,
        2 * rows_here * width * total,
        landing(args),
        range(3),
    )
    arrived = {k: hop(block, distances[k]) for k, block in zip(sent_here, sends)}
    if direct:
        arrived["B"] = lax.ppermute(arrived["A"], "tp", neighbour)

    args = [slots, normed, route_weights.T, shared_gate, shared_up, shared_down]
    sh_send, sh_keep, high, low = call(
        shared_body,
        [shape(rows_here, wide, bf16), shape(rows_here, wide, f32)]
        + [shape(rows_here, total, bf16)] * 2,
        args,
        6 * rows_here * width * shared_gate.shape[1],
        landing(args[2:]),
        range(2, 6),
    )
    sh_came = lax.ppermute(sh_send, "tp", neighbour)

    parties = {"A": ("A",), "B": ("B",), "N": ("P", "Q")} if direct else {"N": ("P",)}
    partner = {"A": "B", "B": "A", "N": "N"}
    kept, came = {}, {}
    for p, names in parties.items():
        send, kept[p] = products([arrived[k] for k in names], [*own, *other], wide)
        came[partner[p]] = lax.ppermute(send, "tp", neighbour)
    returned = {}
    for p, names in parties.items():
        outs = [shape(sizes[k], wide, bf16) for k in names]
        outs = call(add_body, outs, [kept[p], came[p]], came[p].size)
        for k, out in zip(names, outs):
            returned[k] = hop(out, distances[k])

    mine, sent = call(
        functools.partial(mix_body, len(sizes)),
        [shape(rows_here, share, f32), shape(rows_here, share, f32)],
        [high, low, *[returned[k] for k in sizes], sh_keep, sh_came],
        4 * rows_here * wide * total,
        [pltpu.VMEM((total, wide), bf16)],
    )
    came = lax.ppermute(sent, "tp", sibling)
    (mixed,) = call(add_body, [shape(rows_here, share, bf16)], [mine, came], mine.size)
    return mixed


def solution(mesh):
    in_specs = (
        P("ep", None),
        P(),
        P("ep", None),
        P("ep", None),
        P("ep", None, "tp"),
        P("ep", None, "tp"),
        P("ep", "tp", None),
        P(None, "tp"),
        P(None, "tp"),
        P("tp", None),
    )
    out_specs = P("ep", "tp")

    return jax.shard_map(local, mesh=mesh, in_specs=in_specs, out_specs=out_specs, check_vma=False)
```

```python
import functools

import jax
import jax.numpy as jnp
from jax import lax
from jax.experimental import pallas as pl
from jax.experimental.pallas import tpu as pltpu
from jax.sharding import PartitionSpec as P

norm_eps = 1e-06
grant = 16 * 1024 * 1024
f32 = jnp.float32
bf16 = jnp.bfloat16

vmem = pl.BlockSpec(memory_space=pltpu.VMEM)
hbm = pl.BlockSpec(memory_space=pltpu.HBM)


def call(body, outs, ins, flops, scratch=(), far=()):
    moved = sum(a.size * a.dtype.itemsize for a in ins)
    moved += sum(o.size * o.dtype.itemsize for o in outs)
    ins = [
        pltpu.with_memory_space_constraint(a, pltpu.HBM) if i in far else a for i, a in enumerate(ins)
    ]
    return pl.pallas_call(
        body,
        out_shape=outs,
        in_specs=[hbm if i in far else vmem for i in range(len(ins))],
        out_specs=[vmem] * len(outs),
        scratch_shapes=list(scratch),
        compiler_params=pltpu.CompilerParams(vmem_limit_bytes=grant),
        cost_estimate=pl.CostEstimate(flops=flops, bytes_accessed=moved, transcendentals=0),
    )(*ins)


def landing(arrays):
    return [pltpu.VMEM(a.shape, a.dtype) for a in arrays] + [pltpu.SemaphoreType.DMA((len(arrays),))]


def fetch(sources, targets, sems):
    copies = [
        pltpu.make_async_copy(s, t, sems.at[i]) for i, (s, t) in enumerate(zip(sources, targets))
    ]
    for copy in copies:
        copy.start()
    return copies


def shape(rows, columns, dtype):
    return jax.ShapeDtypeStruct((rows, columns), dtype)


def slot_of(label, rank, capacity, direct):
    core, side = lax.axis_index("tp") % 2, lax.axis_index("tp") // 2
    if direct:
        near = label < 4
        holder = jnp.where(near, (label ^ (label >> 1)) & 1, (label >> 1) & 1)
        first = jnp.where((label ^ side) == 4 + 3 * core, 2, 3)
        block = jnp.where(near, label >> 1, first)
        return jnp.where(holder == core, block * capacity + rank, -1)
    half = -(-capacity // 2)
    rank = rank - core * half
    held = jnp.logical_and(rank >= 0, rank < half)
    return jnp.where(held, label * half + rank, -1)


def route_body(capacity, experts, direct, *refs):
    sources, outs, (ids, gain, tokens, sems) = refs[:6], refs[6:-4], refs[-4:]
    copies = fetch(sources, (ids, gain, tokens, *outs[2:5]), sems)
    normed_out, slots_out = outs[0], outs[1]
    rows, width = tokens.shape
    kinds = max(8, experts)
    kind = lax.broadcasted_iota(jnp.int32, (kinds, rows), 0)
    before = (
        lax.broadcasted_iota(jnp.int32, (rows, rows), 0)
        < lax.broadcasted_iota(jnp.int32, (rows, rows), 1)
    ).astype(bf16)
    base = jnp.zeros((kinds, 1), f32)
    total = sum(out.shape[0] for out in outs[5:])
    slot = lax.broadcasted_iota(jnp.int32, (total, rows), 0)
    hit = jnp.zeros((total, rows), f32)
    copies[0].wait()
    for j in range(ids.shape[0]):
        label = ids[j : j + 1, :]
        if direct:
            label = label ^ lax.axis_index("ep")
        onehot = (kind == label).astype(f32)
        earlier = jnp.dot(onehot.astype(bf16), before, preferred_element_type=f32) + base
        rank = jnp.sum(earlier * onehot, axis=0, keepdims=True).astype(jnp.int32)
        base = base + jnp.sum(onehot, axis=1, keepdims=True)
        where = slot_of(label, rank, capacity, direct)
        slots_out[j : j + 1, :] = where
        hit = jnp.where(slot == where, 1.0, hit)
    pick = hit.astype(bf16)
    copies[1].wait()
    copies[2].wait()
    values = tokens[...].astype(f32)
    scale = lax.rsqrt(jnp.mean(values * values, axis=-1, keepdims=True) + norm_eps)
    lanes = gain.shape[1]
    for c in range(width // lanes):
        at = slice(c * lanes, (c + 1) * lanes)
        normed_out[:, at] = (values[:, at] * scale * gain[c : c + 1].astype(f32)).astype(bf16)
    normed = normed_out[...]
    at = 0
    for out in outs[5:]:
        n = out.shape[0]
        part = pick[at : at + n]
        out[...] = jnp.dot(part, normed, preferred_element_type=f32).astype(bf16)
        at += n
    for copy in copies[3:]:
        copy.wait()


def units_of(rows, weights):
    into = [w[...] for w in weights[::3]] + [w[...] for w in weights[1::3]]
    both = jnp.dot(rows, jnp.concatenate(into, axis=1), preferred_element_type=f32)
    units = both.shape[1] // 2
    gate, up = both[:, :units], both[:, units:]
    return (gate / (1.0 + jnp.exp(-gate)) * up).astype(bf16)


def shared_body(slots, rows, *refs):
    weights, gains_in, part, outs = refs[:3], refs[3], refs[4], refs[5:-2]
    gains, sems = refs[-2:]
    (copy,) = fetch((gains_in,), (gains,), sems)
    hidden = units_of(rows[...], weights)
    part[...] = jnp.dot(hidden, weights[2][...], preferred_element_type=f32)
    total = sum(out.shape[1] for out in outs[::2])
    slot = lax.broadcasted_iota(jnp.int32, (total, rows.shape[0]), 0)
    weight = jnp.zeros(slot.shape, f32)
    copy.wait()
    for j in range(slots.shape[0]):
        weight = jnp.where(slot == slots[j : j + 1, :], gains[j : j + 1, :], weight)
    at = 0
    for high_out, low_out in zip(outs[::2], outs[1::2]):
        n = high_out.shape[1]
        turned = weight[at : at + n].T
        high = turned.astype(bf16)
        high_out[...] = high
        low_out[...] = (turned - high.astype(f32)).astype(bf16)
        at += n


def near_body(blocks, *refs):
    rows_in, weights = refs[:blocks], refs[blocks : blocks + 6]
    outs = refs[blocks + 6 : 2 * blocks + 6]
    gathered = gather_rows(rows_in, refs[-1])
    down = jnp.concatenate([w[...] for w in weights[2::3]], axis=0)
    hidden = units_of(gathered[...], weights)
    total = jnp.dot(hidden, down, preferred_element_type=f32).astype(bf16)
    at = 0
    for out in outs:
        out[...] = total[at : at + out.shape[0]]
        at += out.shape[0]


def gather_rows(rows_in, room):
    if len(rows_in) == 1:
        return rows_in[0]
    at = 0
    for ref in rows_in:
        room[at : at + ref.shape[0]] = ref[...]
        at += ref.shape[0]
    return room


def picked(high, low, rows):
    total = jnp.dot(high[...], rows, preferred_element_type=f32)
    return total + jnp.dot(low[...], rows, preferred_element_type=f32)


def first_body(blocks, high, low, part, *refs):
    rows_in, (send, keep) = refs[:blocks], refs[blocks : blocks + 2]
    gathered = gather_rows(rows_in, refs[-1])
    share = keep.shape[1] // 2
    core = lax.axis_index("tp") % 2
    for out, place in ((send, 1 - core), (keep, core)):
        for x in range(2):
            columns = pl.ds(pl.multiple_of((2 * x + place) * share, share), share)
            total = part[:, columns] + picked(high, low, gathered[:, columns])
            out[:, x * share : (x + 1) * share] = total.astype(out.dtype)


def halve_body(keep, came, send, mine):
    share = mine.shape[1]
    side = lax.axis_index("tp") // 2
    for out, place in ((send, 1 - side), (mine, side)):
        columns = pl.ds(pl.multiple_of(place * share, share), share)
        out[...] = (keep[:, columns] + came[:, columns].astype(f32)).astype(out.dtype)


def columns_out(hidden, weights, send, keep):
    side = lax.axis_index("tp") // 2
    width = keep.shape[1]
    for out, place in ((send, 1 - side), (keep, side)):
        columns = pl.ds(pl.multiple_of(place * width, width), width)
        down = jnp.concatenate([w[:, columns] for w in weights[2::3]], axis=0)
        out[...] = jnp.dot(hidden, down, preferred_element_type=f32).astype(out.dtype)


def product_body(*refs):
    rows, weights, send, keep = refs[0], refs[1:7], refs[7], refs[8]
    columns_out(units_of(rows[...], weights), weights, send, keep)


def products(body, rows, weights, outs):
    n = sum(r.shape[0] for r in rows)
    full = rows[0].shape[1]
    hidden = sum(w.shape[1] for w in weights[::3])
    scratch = [pltpu.VMEM((n, full), bf16)] if len(rows) > 1 else []
    return call(body, outs, [*rows, *weights], 6 * n * full * hidden, scratch)


def add_body(keep, came, *outs):
    at = 0
    for out in outs:
        n = out.shape[0]
        out[...] = (keep[at : at + n] + came[at : at + n].astype(f32)).astype(out.dtype)
        at += n


def mix_body(high, low, first, second, mine, came, *refs):
    outs, room = refs[:2], refs[2]
    gathered = gather_rows((first, second), room)
    width = outs[0].shape[1]
    core = lax.axis_index("tp") % 2
    for out, place in ((outs[0], core), (outs[1], 1 - core)):
        columns = pl.ds(pl.multiple_of(place * width, width), width)
        total = picked(high, low, gathered[:, columns])
        out[...] = total + mine[...] + came[...].astype(f32) if out is outs[0] else total


def local(
    tokens,
    norm_gain,
    expert_ids,
    route_weights,
    gate_weight,
    up_weight,
    down_weight,
    shared_gate,
    shared_up,
    shared_down,
):
    rows_here, width = tokens.shape
    chosen = expert_ids.shape[1]
    groups = lax.axis_size("ep")
    cuts = lax.axis_size("tp")
    local_experts = gate_weight.shape[0]
    assert local_experts == 1 and cuts == 4
    capacity = (3 * rows_here * chosen + 2 * groups - 1) // (2 * groups)
    wide, share = width // 2, width // 4
    direct = groups == 8
    sibling = [(i, i ^ 1) for i in range(cuts)]
    neighbour = [(i, i ^ 2) for i in range(cuts)]
    own = (gate_weight[0], up_weight[0], down_weight[0])
    other = tuple(lax.ppermute(w, "tp", sibling) for w in own)

    def hop(block, between):
        if not direct:
            return lax.all_to_all(block, "ep", split_axis=0, concat_axis=0, tiled=True)
        pairs = []
        for i in range(groups):
            for t in range(cuts):
                pairs.append((i * cuts + t, (i ^ between(t // 2, t % 2)) * cuts + t))
        return lax.ppermute(block, ("ep", "tp"), pairs)

    distances = {
        "P": lambda x, c: c,
        "Q": lambda x, c: 3 - c,
        "A": lambda x, c: (4 + 3 * c) ^ x,
        "B": lambda x, c: (4 + 3 * c) ^ x ^ 1,
    }
    half = -(-capacity // 2)
    sizes = {k: capacity for k in distances} if direct else {"P": half * groups}
    sent_here = [k for k in sizes if k != "B"]
    total = sum(sizes.values())
    args = [expert_ids.T, norm_gain.reshape(-1, 128), tokens]
    sh_weights = [shared_gate, shared_up, shared_down]
    normed, slots, *rest = call(
        functools.partial(route_body, capacity, groups, direct),
        [shape(rows_here, width, bf16), shape(chosen, rows_here, jnp.int32)]
        + [shape(*w.shape, w.dtype) for w in sh_weights]
        + [shape(sizes[k], width, bf16) for k in sent_here],
        args + sh_weights,
        2 * rows_here * width * total,
        landing(args)[:-1] + [pltpu.SemaphoreType.DMA((6,))],
        range(6),
    )
    sh_weights, sends = rest[:3], rest[3:]
    arrived = {k: hop(block, distances[k]) for k, block in zip(sent_here, sends)}
    if direct:
        arrived["B"] = lax.ppermute(arrived["A"], "tp", neighbour)
    near = [k for k in sizes if k in ("P", "Q")]
    spans = [sum(sizes[k] for k in near)]
    if direct:
        spans.append(total - spans[0])
    gains = route_weights.T
    part, *weights = call(
        shared_body,
        [shape(rows_here, width, f32)]
        + [shape(rows_here, n, bf16) for n in spans for _ in range(2)],
        [slots, normed, *sh_weights, gains],
        6 * rows_here * width * shared_gate.shape[1],
        landing([gains]),
        [5],
    )

    outs = [shape(sizes[k], width, bf16) for k in near]
    body = functools.partial(near_body, len(near))
    outs = products(body, [arrived[k] for k in near], [*own, *other], outs)
    returned = {k: hop(out, distances[k]) for k, out in zip(near, outs)}
    send, keep = call(
        functools.partial(first_body, len(near)),
        [shape(rows_here, wide, bf16), shape(rows_here, wide, f32)],
        [*weights[:2], part, *[returned[k] for k in near]],
        4 * rows_here * width * spans[0],
        [pltpu.VMEM((spans[0], width), bf16)] if direct else [],
    )
    send, mine = call(
        halve_body,
        [shape(rows_here, share, bf16), shape(rows_here, share, f32)],
        [keep, lax.ppermute(send, "tp", sibling)],
        keep.size,
    )
    came = lax.ppermute(send, "tp", neighbour)

    if direct:
        sent, kept = {}, {}
        for k in "AB":
            outs = [shape(capacity, wide, bf16), shape(capacity, wide, f32)]
            sent[k], kept[k] = products(product_body, [arrived[k]], [*own, *other], outs)
            sent[k] = lax.ppermute(sent[k], "tp", neighbour)
        for k, other_k in ("AB", "BA"):
            ins = [kept[k], sent[other_k]]
            (out,) = call(add_body, [shape(capacity, wide, bf16)], ins, kept[k].size)
            returned[k] = hop(out, distances[k])
        mine, send = call(
            mix_body,
            [shape(rows_here, share, f32), shape(rows_here, share, f32)],
            [*weights[2:], returned["A"], returned["B"], mine, came],
            4 * rows_here * wide * spans[1],
            [pltpu.VMEM((spans[1], wide), bf16)],
        )
        came = lax.ppermute(send, "tp", sibling)
    (mixed,) = call(add_body, [shape(rows_here, share, bf16)], [mine, came], mine.size)
    return mixed


def solution(mesh):
    in_specs = (
        P("ep", None),
        P(),
        P("ep", None),
        P("ep", None),
        P("ep", None, "tp"),
        P("ep", None, "tp"),
        P("ep", "tp", None),
        P(None, "tp"),
        P(None, "tp"),
        P("tp", None),
    )
    out_specs = P("ep", "tp")

    return jax.shard_map(local, mesh=mesh, in_specs=in_specs, out_specs=out_specs, check_vma=False)
```

```python
import functools

import jax
import jax.numpy as jnp
from jax import lax
from jax.experimental import pallas as pl
from jax.experimental.pallas import tpu as pltpu
from jax.sharding import PartitionSpec as P

norm_eps = 1e-06
grant = 16 * 1024 * 1024
f32 = jnp.float32
bf16 = jnp.bfloat16

vmem = pl.BlockSpec(memory_space=pltpu.VMEM)
hbm = pl.BlockSpec(memory_space=pltpu.HBM)


def call(body, outs, ins, flops, scratch=(), far=()):
    moved = sum(a.size * a.dtype.itemsize for a in ins)
    moved += sum(o.size * o.dtype.itemsize for o in outs)
    ins = [
        pltpu.with_memory_space_constraint(a, pltpu.HBM) if i in far else a for i, a in enumerate(ins)
    ]
    return pl.pallas_call(
        body,
        out_shape=outs,
        in_specs=[hbm if i in far else vmem for i in range(len(ins))],
        out_specs=[vmem] * len(outs),
        scratch_shapes=list(scratch),
        compiler_params=pltpu.CompilerParams(vmem_limit_bytes=grant),
        cost_estimate=pl.CostEstimate(flops=flops, bytes_accessed=moved, transcendentals=0),
    )(*ins)


def landing(arrays):
    return [pltpu.VMEM(a.shape, a.dtype) for a in arrays] + [pltpu.SemaphoreType.DMA((len(arrays),))]


def fetch(sources, targets, sems):
    copies = [
        pltpu.make_async_copy(s, t, sems.at[i]) for i, (s, t) in enumerate(zip(sources, targets))
    ]
    for copy in copies:
        copy.start()
    return copies


def shape(rows, columns, dtype):
    return jax.ShapeDtypeStruct((rows, columns), dtype)


def slot_of(label, rank, capacity, direct, flip=0):
    core, side = (lax.axis_index("tp") % 2) ^ flip, lax.axis_index("tp") // 2
    if direct:
        near = label < 4
        holder = jnp.where(near, (label ^ (label >> 1)) & 1, (label >> 1) & 1)
        first = jnp.where((label ^ side) == 4 + 3 * core, 2, 3)
        block = jnp.where(near, label >> 1, first)
        return jnp.where(holder == core, block * capacity + rank, -1)
    half = -(-capacity // 2)
    rank = rank - core * half
    held = jnp.logical_and(rank >= 0, rank < half)
    return jnp.where(held, label * half + rank, -1)


def route_body(capacity, experts, direct, *refs):
    sources, outs, (ids, gain, tokens, sems) = refs[:6], refs[6:-4], refs[-4:]
    copies = fetch(sources, (ids, gain, tokens, *outs[2:5]), sems)
    normed_out, slots_out = outs[0], outs[1]
    rows, width = tokens.shape
    kinds = max(8, experts)
    kind = lax.broadcasted_iota(jnp.int32, (kinds, rows), 0)
    before = (
        lax.broadcasted_iota(jnp.int32, (rows, rows), 0)
        < lax.broadcasted_iota(jnp.int32, (rows, rows), 1)
    ).astype(bf16)
    base = jnp.zeros((kinds, 1), f32)
    total = sum(out.shape[0] for out in outs[5:])
    slot = lax.broadcasted_iota(jnp.int32, (total, rows), 0)
    hit = jnp.zeros((total, rows), f32)
    copies[0].wait()
    for j in range(ids.shape[0]):
        label = ids[j : j + 1, :]
        if direct:
            label = label ^ lax.axis_index("ep")
        onehot = (kind == label).astype(f32)
        earlier = jnp.dot(onehot.astype(bf16), before, preferred_element_type=f32) + base
        rank = jnp.sum(earlier * onehot, axis=0, keepdims=True).astype(jnp.int32)
        base = base + jnp.sum(onehot, axis=1, keepdims=True)
        where = slot_of(label, rank, capacity, direct)
        slots_out[j : j + 1, :] = where
        if direct:
            there = slot_of(label, rank, capacity, direct, 1)
            there = jnp.where(there >= 2 * capacity, there + 2 * capacity, -1)
            slots_out[j : j + 1, :] = jnp.maximum(where, there)
        hit = jnp.where(slot == where, 1.0, hit)
    pick = hit.astype(bf16)
    copies[1].wait()
    copies[2].wait()
    values = tokens[...].astype(f32)
    scale = lax.rsqrt(jnp.mean(values * values, axis=-1, keepdims=True) + norm_eps)
    lanes = gain.shape[1]
    for c in range(width // lanes):
        at = slice(c * lanes, (c + 1) * lanes)
        normed_out[:, at] = (values[:, at] * scale * gain[c : c + 1].astype(f32)).astype(bf16)
    normed = normed_out[...]
    at = 0
    for out in outs[5:]:
        n = out.shape[0]
        part = pick[at : at + n]
        out[...] = jnp.dot(part, normed, preferred_element_type=f32).astype(bf16)
        at += n
    for copy in copies[3:]:
        copy.wait()


def units_of(rows, weights):
    into = [w[...] for w in weights[::3]] + [w[...] for w in weights[1::3]]
    both = jnp.dot(rows, jnp.concatenate(into, axis=1), preferred_element_type=f32)
    units = both.shape[1] // 2
    gate, up = both[:, :units], both[:, units:]
    return (gate / (1.0 + jnp.exp(-gate)) * up).astype(bf16)


def shared_body(slots, rows, *refs):
    weights, gains_in, part, outs = refs[:3], refs[3], refs[4], refs[5:-2]
    gains, sems = refs[-2:]
    (copy,) = fetch((gains_in,), (gains,), sems)
    hidden = units_of(rows[...], weights)
    part[...] = jnp.dot(hidden, weights[2][...], preferred_element_type=f32)
    total = sum(out.shape[1] for out in outs[::2])
    slot = lax.broadcasted_iota(jnp.int32, (total, rows.shape[0]), 0)
    weight = jnp.zeros(slot.shape, f32)
    copy.wait()
    for j in range(slots.shape[0]):
        weight = jnp.where(slot == slots[j : j + 1, :], gains[j : j + 1, :], weight)
    at = 0
    for high_out, low_out in zip(outs[::2], outs[1::2]):
        n = high_out.shape[1]
        turned = weight[at : at + n].T
        high = turned.astype(bf16)
        high_out[...] = high
        low_out[...] = (turned - high.astype(f32)).astype(bf16)
        at += n


def near_body(blocks, *refs):
    rows_in, weights = refs[:blocks], refs[blocks : blocks + 6]
    outs = refs[blocks + 6 : 2 * blocks + 6]
    gathered = gather_rows(rows_in, refs[-1])
    down = jnp.concatenate([w[...] for w in weights[2::3]], axis=0)
    hidden = units_of(gathered[...], weights)
    total = jnp.dot(hidden, down, preferred_element_type=f32).astype(bf16)
    at = 0
    for out in outs:
        out[...] = total[at : at + out.shape[0]]
        at += out.shape[0]


def gather_rows(rows_in, room):
    if len(rows_in) == 1:
        return rows_in[0]
    at = 0
    for ref in rows_in:
        room[at : at + ref.shape[0]] = ref[...]
        at += ref.shape[0]
    return room


def picked(high, low, rows):
    total = jnp.dot(high[...], rows, preferred_element_type=f32)
    return total + jnp.dot(low[...], rows, preferred_element_type=f32)


def first_body(blocks, high, low, part, *refs):
    rows_in, (send, keep) = refs[:blocks], refs[blocks : blocks + 2]
    gathered = gather_rows(rows_in, refs[-1])
    share = keep.shape[1] // 2
    core = lax.axis_index("tp") % 2
    for out, place in ((send, 1 - core), (keep, core)):
        for x in range(2):
            columns = pl.ds(pl.multiple_of((2 * x + place) * share, share), share)
            total = part[:, columns] + picked(high, low, gathered[:, columns])
            out[:, x * share : (x + 1) * share] = total.astype(out.dtype)


def halve_body(keep, came, send, mine):
    share = mine.shape[1]
    side = lax.axis_index("tp") // 2
    for out, place in ((send, 1 - side), (mine, side)):
        columns = pl.ds(pl.multiple_of(place * share, share), share)
        out[...] = (keep[:, columns] + came[:, columns].astype(f32)).astype(out.dtype)


def columns_out(hidden, weights, send, keep):
    side = lax.axis_index("tp") // 2
    width = keep.shape[1]
    for out, place in ((send, 1 - side), (keep, side)):
        columns = pl.ds(pl.multiple_of(place * width, width), width)
        down = jnp.concatenate([w[:, columns] for w in weights[2::3]], axis=0)
        out[...] = jnp.dot(hidden, down, preferred_element_type=f32).astype(out.dtype)


def product_body(*refs):
    rows, weights, send, keep = refs[0], refs[1:7], refs[7], refs[8]
    columns_out(units_of(rows[...], weights), weights, send, keep)


def products(body, rows, weights, outs):
    n = sum(r.shape[0] for r in rows)
    full = rows[0].shape[1]
    hidden = sum(w.shape[1] for w in weights[::3])
    scratch = [pltpu.VMEM((n, full), bf16)] if len(rows) > 1 else []
    return call(body, outs, [*rows, *weights], 6 * n * full * hidden, scratch)


def add_body(keep, came, *outs):
    if len(outs) == 1:
        outs[0][...] = (keep[...] + came[...].astype(f32)).astype(outs[0].dtype)
        return
    width = outs[0].shape[1]
    core = lax.axis_index("tp") % 2
    for out, place in ((outs[0], core), (outs[1], 1 - core)):
        columns = pl.ds(pl.multiple_of(place * width, width), width)
        out[...] = (keep[:, columns] + came[:, columns].astype(f32)).astype(out.dtype)


def mix_body(high, low, mine, came, *refs):
    out, room = refs[-2:]
    rows = gather_rows(refs[:-2], room)[...]
    out[...] = (picked(high, low, rows) + mine[...] + came[...].astype(f32)).astype(out.dtype)


def local(
    tokens,
    norm_gain,
    expert_ids,
    route_weights,
    gate_weight,
    up_weight,
    down_weight,
    shared_gate,
    shared_up,
    shared_down,
):
    rows_here, width = tokens.shape
    chosen = expert_ids.shape[1]
    groups = lax.axis_size("ep")
    cuts = lax.axis_size("tp")
    local_experts = gate_weight.shape[0]
    assert local_experts == 1 and cuts == 4
    capacity = (3 * rows_here * chosen + 2 * groups - 1) // (2 * groups)
    wide, share = width // 2, width // 4
    direct = groups == 8
    sibling = [(i, i ^ 1) for i in range(cuts)]
    neighbour = [(i, i ^ 2) for i in range(cuts)]
    own = (gate_weight[0], up_weight[0], down_weight[0])
    other = tuple(lax.ppermute(w, "tp", sibling) for w in own)

    def hop(block, between, flip=0):
        if not direct:
            return lax.all_to_all(block, "ep", split_axis=0, concat_axis=0, tiled=True)
        pairs = []
        for i in range(groups):
            for t in range(cuts):
                to = i ^ between(t // 2, t % 2)
                pairs.append((i * cuts + t, to * cuts + (t ^ flip)))
        return lax.ppermute(block, ("ep", "tp"), pairs)

    distances = {
        "P": lambda x, c: c,
        "Q": lambda x, c: 3 - c,
        "A": lambda x, c: (4 + 3 * c) ^ x,
        "B": lambda x, c: (4 + 3 * c) ^ x ^ 1,
    }
    half = -(-capacity // 2)
    sizes = {k: capacity for k in distances} if direct else {"P": half * groups}
    sent_here = [k for k in sizes if k != "B"]
    total = sum(sizes.values())
    args = [expert_ids.T, norm_gain.reshape(-1, 128), tokens]
    sh_weights = [shared_gate, shared_up, shared_down]
    normed, slots, *rest = call(
        functools.partial(route_body, capacity, groups, direct),
        [shape(rows_here, width, bf16), shape(chosen, rows_here, jnp.int32)]
        + [shape(*w.shape, w.dtype) for w in sh_weights]
        + [shape(sizes[k], width, bf16) for k in sent_here],
        args + sh_weights,
        2 * rows_here * width * total,
        landing(args)[:-1] + [pltpu.SemaphoreType.DMA((6,))],
        range(6),
    )
    sh_weights, sends = rest[:3], rest[3:]
    arrived = {k: hop(block, distances[k]) for k, block in zip(sent_here, sends)}
    if direct:
        arrived["B"] = lax.ppermute(arrived["A"], "tp", neighbour)
    near = [k for k in sizes if k in ("P", "Q")]
    spans = [sum(sizes[k] for k in near)]
    if direct:
        spans.append(2 * (total - spans[0]))
    gains = route_weights.T
    part, *weights = call(
        shared_body,
        [shape(rows_here, width, f32)]
        + [shape(rows_here, n, bf16) for n in spans for _ in range(2)],
        [slots, normed, *sh_weights, gains],
        6 * rows_here * width * shared_gate.shape[1],
        landing([gains]),
        [5],
    )

    outs = [shape(sizes[k], width, bf16) for k in near]
    body = functools.partial(near_body, len(near))
    outs = products(body, [arrived[k] for k in near], [*own, *other], outs)
    returned = {k: hop(out, distances[k]) for k, out in zip(near, outs)}
    send, keep = call(
        functools.partial(first_body, len(near)),
        [shape(rows_here, wide, bf16), shape(rows_here, wide, f32)],
        [*weights[:2], part, *[returned[k] for k in near]],
        4 * rows_here * width * spans[0],
        [pltpu.VMEM((spans[0], width), bf16)] if direct else [],
    )
    send, mine = call(
        halve_body,
        [shape(rows_here, share, bf16), shape(rows_here, share, f32)],
        [keep, lax.ppermute(send, "tp", sibling)],
        keep.size,
    )
    came = lax.ppermute(send, "tp", neighbour)

    if direct:
        sent, kept = {}, {}
        for k in "AB":
            outs = [shape(capacity, wide, bf16), shape(capacity, wide, f32)]
            sent[k], kept[k] = products(product_body, [arrived[k]], [*own, *other], outs)
            sent[k] = lax.ppermute(sent[k], "tp", neighbour)
        far_rows = {}
        for k, other_k in ("AB", "BA"):
            ins = [kept[k], sent[other_k]]
            outs = [shape(capacity, share, bf16)] * 2
            outs = call(add_body, outs, ins, kept[k].size)
            for flip, out in enumerate(outs):
                far_rows[k, flip] = hop(out, distances[k], flip)
        rows = [far_rows[k, flip] for flip in range(2) for k in "AB"]
        (mixed,) = call(
            mix_body,
            [shape(rows_here, share, bf16)],
            [*weights[2:], mine, came, *rows],
            4 * rows_here * share * spans[1],
            [pltpu.VMEM((spans[1], share), bf16)],
        )
        return mixed
    (mixed,) = call(add_body, [shape(rows_here, share, bf16)], [mine, came], mine.size)
    return mixed


def solution(mesh):
    in_specs = (
        P("ep", None),
        P(),
        P("ep", None),
        P("ep", None),
        P("ep", None, "tp"),
        P("ep", None, "tp"),
        P("ep", "tp", None),
        P(None, "tp"),
        P(None, "tp"),
        P("tp", None),
    )
    out_specs = P("ep", "tp")

    return jax.shard_map(local, mesh=mesh, in_specs=in_specs, out_specs=out_specs, check_vma=False)
```

```python
import functools

import jax
import jax.numpy as jnp
from jax import lax
from jax.experimental import pallas as pl
from jax.experimental.pallas import tpu as pltpu
from jax.sharding import PartitionSpec as P

norm_eps = 1e-06
grant = 16 * 1024 * 1024
f32 = jnp.float32
bf16 = jnp.bfloat16

vmem = pl.BlockSpec(memory_space=pltpu.VMEM)
hbm = pl.BlockSpec(memory_space=pltpu.HBM)


def call(body, outs, ins, flops, scratch=(), far=()):
    moved = sum(a.size * a.dtype.itemsize for a in ins)
    moved += sum(o.size * o.dtype.itemsize for o in outs)
    ins = [
        pltpu.with_memory_space_constraint(a, pltpu.HBM) if i in far else a for i, a in enumerate(ins)
    ]
    return pl.pallas_call(
        body,
        out_shape=outs,
        in_specs=[hbm if i in far else vmem for i in range(len(ins))],
        out_specs=[vmem] * len(outs),
        scratch_shapes=list(scratch),
        compiler_params=pltpu.CompilerParams(vmem_limit_bytes=grant),
        cost_estimate=pl.CostEstimate(flops=flops, bytes_accessed=moved, transcendentals=0),
    )(*ins)


def landing(arrays):
    return [pltpu.VMEM(a.shape, a.dtype) for a in arrays] + [pltpu.SemaphoreType.DMA((len(arrays),))]


def fetch(sources, targets, sems):
    copies = [
        pltpu.make_async_copy(s, t, sems.at[i]) for i, (s, t) in enumerate(zip(sources, targets))
    ]
    for copy in copies:
        copy.start()
    return copies


def shape(rows, columns, dtype):
    return jax.ShapeDtypeStruct((rows, columns), dtype)


def slot_of(label, rank, capacity, direct, flip=0):
    core, side = (lax.axis_index("tp") % 2) ^ flip, lax.axis_index("tp") // 2
    if direct:
        near = label < 4
        holder = jnp.where(near, (label ^ (label >> 1)) & 1, (label >> 1) & 1)
        first = jnp.where((label ^ side) == 4 + 3 * core, 2, 3)
        block = jnp.where(near, label >> 1, first)
        return jnp.where(holder == core, block * capacity + rank, -1)
    half = -(-capacity // 2)
    rank = rank - core * half
    held = jnp.logical_and(rank >= 0, rank < half)
    return jnp.where(held, label * half + rank, -1)


def route_body(capacity, experts, direct, *refs):
    sources, outs, (ids, gain, tokens, sems) = refs[:6], refs[6:-4], refs[-4:]
    copies = fetch(sources, (ids, gain, tokens, *outs[2:5]), sems)
    normed_out, slots_out = outs[0], outs[1]
    rows, width = tokens.shape
    kinds = max(8, experts)
    kind = lax.broadcasted_iota(jnp.int32, (kinds, rows), 0)
    before = (
        lax.broadcasted_iota(jnp.int32, (rows, rows), 0)
        < lax.broadcasted_iota(jnp.int32, (rows, rows), 1)
    ).astype(bf16)
    base = jnp.zeros((kinds, 1), f32)
    total = sum(out.shape[0] for out in outs[5:])
    slot = lax.broadcasted_iota(jnp.int32, (total, rows), 0)
    hit = jnp.zeros((total, rows), f32)
    copies[0].wait()
    for j in range(ids.shape[0]):
        label = ids[j : j + 1, :]
        if direct:
            label = label ^ lax.axis_index("ep")
        onehot = (kind == label).astype(f32)
        earlier = jnp.dot(onehot.astype(bf16), before, preferred_element_type=f32) + base
        rank = jnp.sum(earlier * onehot, axis=0, keepdims=True).astype(jnp.int32)
        base = base + jnp.sum(onehot, axis=1, keepdims=True)
        where = slot_of(label, rank, capacity, direct)
        slots_out[j : j + 1, :] = where
        if direct:
            there = slot_of(label, rank, capacity, direct, 1)
            own_far = jnp.logical_and(there >= 2 * capacity, there < 3 * capacity)
            there = jnp.where(own_far, there + 2 * capacity, -1)
            slots_out[j : j + 1, :] = jnp.maximum(where, there)
        hit = jnp.where(slot == where, 1.0, hit)
    pick = hit.astype(bf16)
    copies[1].wait()
    copies[2].wait()
    values = tokens[...].astype(f32)
    scale = lax.rsqrt(jnp.mean(values * values, axis=-1, keepdims=True) + norm_eps)
    lanes = gain.shape[1]
    for c in range(width // lanes):
        at = slice(c * lanes, (c + 1) * lanes)
        normed_out[:, at] = (values[:, at] * scale * gain[c : c + 1].astype(f32)).astype(bf16)
    normed = normed_out[...]
    at = 0
    for out in outs[5:]:
        n = out.shape[0]
        part = pick[at : at + n]
        out[...] = jnp.dot(part, normed, preferred_element_type=f32).astype(bf16)
        at += n
    for copy in copies[3:]:
        copy.wait()


def units_of(rows, weights):
    into = [w[...] for w in weights[::3]] + [w[...] for w in weights[1::3]]
    both = jnp.dot(rows, jnp.concatenate(into, axis=1), preferred_element_type=f32)
    units = both.shape[1] // 2
    gate, up = both[:, :units], both[:, units:]
    return (gate / (1.0 + jnp.exp(-gate)) * up).astype(bf16)


def shared_body(groups, total, slots, rows, *refs):
    weights, gains_in, part, outs = refs[:3], refs[3], refs[4], refs[5:-2]
    gains, sems = refs[-2:]
    (copy,) = fetch((gains_in,), (gains,), sems)
    hidden = units_of(rows[...], weights)
    part[...] = jnp.dot(hidden, weights[2][...], preferred_element_type=f32)
    slot = lax.broadcasted_iota(jnp.int32, (total, rows.shape[0]), 0)
    weight = jnp.zeros(slot.shape, f32)
    copy.wait()
    for j in range(slots.shape[0]):
        weight = jnp.where(slot == slots[j : j + 1, :], gains[j : j + 1, :], weight)
    high = weight.astype(bf16).astype(f32)
    low = weight - high
    for out, spans in zip(outs, groups):
        parts = [half[a:b] for a, b in spans for half in (high, low)]
        out[...] = jnp.concatenate(parts, axis=0).T.astype(bf16)


def near_body(blocks, *refs):
    rows_in, weights = refs[:blocks], refs[blocks : blocks + 6]
    outs = refs[blocks + 6 : 2 * blocks + 6]
    gathered = gather_rows(rows_in, refs[-1])
    down = jnp.concatenate([w[...] for w in weights[2::3]], axis=0)
    hidden = units_of(gathered[...], weights)
    total = jnp.dot(hidden, down, preferred_element_type=f32).astype(bf16)
    at = 0
    for out in outs:
        out[...] = total[at : at + out.shape[0]]
        at += out.shape[0]


def gather_rows(rows_in, room):
    if len(rows_in) == 1:
        return rows_in[0]
    at = 0
    for ref in rows_in:
        room[at : at + ref.shape[0]] = ref[...]
        at += ref.shape[0]
    return room


def picked(weights, rows):
    return jnp.dot(weights[...], rows, preferred_element_type=f32)


def first_body(blocks, weights, part, *refs):
    rows_in, (send, keep) = refs[:blocks], refs[blocks : blocks + 2]
    gathered = gather_rows((*rows_in, *rows_in), refs[-1])
    share = keep.shape[1] // 2
    core = lax.axis_index("tp") % 2
    for out, place in ((send, 1 - core), (keep, core)):
        for x in range(2):
            columns = pl.ds(pl.multiple_of((2 * x + place) * share, share), share)
            total = part[:, columns] + picked(weights, gathered[:, columns])
            out[:, x * share : (x + 1) * share] = total.astype(out.dtype)


def halve_body(keep, came, send, mine):
    share = mine.shape[1]
    side = lax.axis_index("tp") // 2
    for out, place in ((send, 1 - side), (mine, side)):
        columns = pl.ds(pl.multiple_of(place * share, share), share)
        out[...] = (keep[:, columns] + came[:, columns].astype(f32)).astype(out.dtype)


def columns_out(hidden, weights, send, keep):
    side = lax.axis_index("tp") // 2
    width = keep.shape[1]
    for out, place in ((send, 1 - side), (keep, side)):
        columns = pl.ds(pl.multiple_of(place * width, width), width)
        down = jnp.concatenate([w[:, columns] for w in weights[2::3]], axis=0)
        out[...] = jnp.dot(hidden, down, preferred_element_type=f32).astype(out.dtype)


def product_body(*refs):
    rows, weights, send, keep = refs[0], refs[1:7], refs[7], refs[8]
    columns_out(units_of(rows[...], weights), weights, send, keep)


def products(body, rows, weights, outs):
    n = sum(r.shape[0] for r in rows)
    full = rows[0].shape[1]
    hidden = sum(w.shape[1] for w in weights[::3])
    scratch = [pltpu.VMEM((n, full), bf16)] if len(rows) > 1 else []
    return call(body, outs, [*rows, *weights], 6 * n * full * hidden, scratch)


def add_body(keep, came, *outs):
    if len(outs) == 1:
        outs[0][...] = (keep[...] + came[...].astype(f32)).astype(outs[0].dtype)
        return
    width = outs[0].shape[1]
    core = lax.axis_index("tp") % 2
    for out, place in ((outs[0], core), (outs[1], 1 - core)):
        columns = pl.ds(pl.multiple_of(place * width, width), width)
        out[...] = (keep[:, columns] + came[:, columns].astype(f32)).astype(out.dtype)


def swap_body(weights, rows, mine, send, keep, room):
    gathered = gather_rows((rows, rows), room)
    width = keep.shape[1]
    core = lax.axis_index("tp") % 2
    columns = pl.ds(pl.multiple_of((1 - core) * width, width), width)
    send[...] = picked(weights, gathered[:, columns])
    columns = pl.ds(pl.multiple_of(core * width, width), width)
    keep[...] = picked(weights, gathered[:, columns]) + mine[...]


def mix_body(weights, rows, rows2, came, kept, swapped, out, room):
    gathered = gather_rows((rows, rows, rows2, rows2), room)
    total = came[...].astype(f32) + kept[...] + swapped[...]
    out[...] = (total + picked(weights, gathered[...])).astype(out.dtype)


def local(
    tokens,
    norm_gain,
    expert_ids,
    route_weights,
    gate_weight,
    up_weight,
    down_weight,
    shared_gate,
    shared_up,
    shared_down,
):
    rows_here, width = tokens.shape
    chosen = expert_ids.shape[1]
    groups = lax.axis_size("ep")
    cuts = lax.axis_size("tp")
    local_experts = gate_weight.shape[0]
    assert local_experts == 1 and cuts == 4
    capacity = (3 * rows_here * chosen + 2 * groups - 1) // (2 * groups)
    wide, share = width // 2, width // 4
    direct = groups == 8
    sibling = [(i, i ^ 1) for i in range(cuts)]
    neighbour = [(i, i ^ 2) for i in range(cuts)]
    own = (gate_weight[0], up_weight[0], down_weight[0])
    other = tuple(lax.ppermute(w, "tp", sibling) for w in own)

    def hop(block, between, flip=0):
        if not direct:
            return lax.all_to_all(block, "ep", split_axis=0, concat_axis=0, tiled=True)
        pairs = []
        for i in range(groups):
            for t in range(cuts):
                to = i ^ between(t // 2, t % 2)
                pairs.append((i * cuts + t, to * cuts + (t ^ flip)))
        return lax.ppermute(block, ("ep", "tp"), pairs)

    distances = {
        "P": lambda x, c: c,
        "Q": lambda x, c: 3 - c,
        "A": lambda x, c: (4 + 3 * c) ^ x,
        "B": lambda x, c: (4 + 3 * c) ^ x ^ 1,
    }
    half = -(-capacity // 2)
    sizes = {k: capacity for k in distances} if direct else {"P": half * groups}
    sent_here = [k for k in sizes if k != "B"]
    total = sum(sizes.values())
    args = [expert_ids.T, norm_gain.reshape(-1, 128), tokens]
    sh_weights = [shared_gate, shared_up, shared_down]
    normed, slots, *rest = call(
        functools.partial(route_body, capacity, groups, direct),
        [shape(rows_here, width, bf16), shape(chosen, rows_here, jnp.int32)]
        + [shape(*w.shape, w.dtype) for w in sh_weights]
        + [shape(sizes[k], width, bf16) for k in sent_here],
        args + sh_weights,
        2 * rows_here * width * total,
        landing(args)[:-1] + [pltpu.SemaphoreType.DMA((6,))],
        range(6),
    )
    sh_weights, sends = rest[:3], rest[3:]
    arrived = {k: hop(block, distances[k]) for k, block in zip(sent_here, sends)}
    if direct:
        arrived["B"] = lax.ppermute(arrived["A"], "tp", neighbour)
    near = [k for k in sizes if k in ("P", "Q")]
    n_near = sum(sizes[k] for k in near)
    groups_of = [[(0, n_near)]]
    if direct:
        at = [i * capacity for i in range(6)]
        groups_of += [[(at[3], at[4])], [(at[2], at[3]), (at[4], at[5])]]
        total = at[5]
    gains = route_weights.T
    part, *weights = call(
        functools.partial(shared_body, groups_of, total),
        [shape(rows_here, width, f32)]
        + [shape(rows_here, 2 * sum(b - a for a, b in spans), bf16) for spans in groups_of],
        [slots, normed, *sh_weights, gains],
        6 * rows_here * width * shared_gate.shape[1],
        landing([gains]),
        [5],
    )

    outs = [shape(sizes[k], width, bf16) for k in near]
    body = functools.partial(near_body, len(near))
    outs = products(body, [arrived[k] for k in near], [*own, *other], outs)
    returned = {k: hop(out, distances[k]) for k, out in zip(near, outs)}
    send, keep = call(
        functools.partial(first_body, len(near)),
        [shape(rows_here, wide, bf16), shape(rows_here, wide, f32)],
        [weights[0], part, *[returned[k] for k in near]],
        4 * rows_here * width * n_near,
        [pltpu.VMEM((2 * n_near, width), bf16)],
    )
    send, mine = call(
        halve_body,
        [shape(rows_here, share, bf16), shape(rows_here, share, f32)],
        [keep, lax.ppermute(send, "tp", sibling)],
        keep.size,
    )
    came = lax.ppermute(send, "tp", neighbour)

    if direct:
        sent, kept = {}, {}
        for k in "AB":
            outs = [shape(capacity, wide, bf16), shape(capacity, wide, f32)]
            sent[k], kept[k] = products(product_body, [arrived[k]], [*own, *other], outs)
            sent[k] = lax.ppermute(sent[k], "tp", neighbour)
        ins, outs = [kept["B"], sent["A"]], [shape(capacity, wide, bf16)]
        (out,) = call(add_body, outs, ins, kept["B"].size)
        out = hop(out, distances["B"])
        send, swap_mine = call(
            swap_body,
            [shape(rows_here, share, f32)] * 2,
            [weights[1], out, mine],
            4 * rows_here * wide * capacity,
            [pltpu.VMEM((2 * capacity, wide), bf16)],
        )
        swap_came = lax.ppermute(send, "tp", sibling)
        ins, outs = [kept["A"], sent["B"]], [shape(capacity, share, bf16)] * 2
        outs = call(add_body, outs, ins, kept["A"].size)
        rows = [hop(out, distances["A"], flip) for flip, out in enumerate(outs)]
        (mixed,) = call(
            mix_body,
            [shape(rows_here, share, bf16)],
            [weights[2], *rows, came, swap_mine, swap_came],
            8 * rows_here * share * capacity,
            [pltpu.VMEM((4 * capacity, share), bf16)],
        )
        return mixed
    (mixed,) = call(add_body, [shape(rows_here, share, bf16)], [mine, came], mine.size)
    return mixed


def solution(mesh):
    in_specs = (
        P("ep", None),
        P(),
        P("ep", None),
        P("ep", None),
        P("ep", None, "tp"),
        P("ep", None, "tp"),
        P("ep", "tp", None),
        P(None, "tp"),
        P(None, "tp"),
        P("tp", None),
    )
    out_specs = P("ep", "tp")

    return jax.shard_map(local, mesh=mesh, in_specs=in_specs, out_specs=out_specs, check_vma=False)
```

```python
import functools

import jax
import jax.numpy as jnp
from jax import lax
from jax.experimental import pallas as pl
from jax.experimental.pallas import tpu as pltpu
from jax.sharding import PartitionSpec as P

norm_eps = 1e-06
grant = 16 * 1024 * 1024
f32 = jnp.float32
bf16 = jnp.bfloat16

vmem = pl.BlockSpec(memory_space=pltpu.VMEM)
hbm = pl.BlockSpec(memory_space=pltpu.HBM)


def call(body, outs, ins, flops, scratch=(), far=()):
    moved = sum(a.size * a.dtype.itemsize for a in ins)
    moved += sum(o.size * o.dtype.itemsize for o in outs)
    ins = [
        pltpu.with_memory_space_constraint(a, pltpu.HBM) if i in far else a for i, a in enumerate(ins)
    ]
    return pl.pallas_call(
        body,
        out_shape=outs,
        in_specs=[hbm if i in far else vmem for i in range(len(ins))],
        out_specs=[vmem] * len(outs),
        scratch_shapes=list(scratch),
        compiler_params=pltpu.CompilerParams(vmem_limit_bytes=grant),
        cost_estimate=pl.CostEstimate(flops=flops, bytes_accessed=moved, transcendentals=0),
    )(*ins)


def landing(arrays):
    return [pltpu.VMEM(a.shape, a.dtype) for a in arrays] + [pltpu.SemaphoreType.DMA((len(arrays),))]


def fetch(sources, targets, sems):
    copies = [
        pltpu.make_async_copy(s, t, sems.at[i]) for i, (s, t) in enumerate(zip(sources, targets))
    ]
    for copy in copies:
        copy.start()
    return copies


def shape(rows, columns, dtype):
    return jax.ShapeDtypeStruct((rows, columns), dtype)


def slot_of(label, rank, capacity, direct, flip=0):
    core, side = (lax.axis_index("tp") % 2) ^ flip, lax.axis_index("tp") // 2
    if direct:
        near = label < 4
        holder = jnp.where(near, (label ^ (label >> 1)) & 1, (label >> 1) & 1)
        first = jnp.where((label ^ side) == 4 + 3 * core, 2, 3)
        block = jnp.where(near, label >> 1, first)
        return jnp.where(holder == core, block * capacity + rank, -1)
    half = -(-capacity // 2)
    rank = rank - core * half
    held = jnp.logical_and(rank >= 0, rank < half)
    return jnp.where(held, label * half + rank, -1)


def route_body(capacity, experts, direct, *refs):
    sources, outs, (ids, gain, tokens, sems) = refs[:3], refs[3:-4], refs[-4:]
    copies = fetch(sources, (ids, gain, tokens), sems)
    normed_out, slots_out = outs[0], outs[1]
    rows, width = tokens.shape
    kinds = max(8, experts)
    kind = lax.broadcasted_iota(jnp.int32, (kinds, rows), 0)
    before = (
        lax.broadcasted_iota(jnp.int32, (rows, rows), 0)
        < lax.broadcasted_iota(jnp.int32, (rows, rows), 1)
    ).astype(bf16)
    base = jnp.zeros((kinds, 1), f32)
    total = sum(out.shape[0] for out in outs[2:])
    slot = lax.broadcasted_iota(jnp.int32, (total, rows), 0)
    hit = jnp.zeros((total, rows), f32)
    copies[0].wait()
    for j in range(ids.shape[0]):
        label = ids[j : j + 1, :]
        if direct:
            label = label ^ lax.axis_index("ep")
        onehot = (kind == label).astype(f32)
        earlier = jnp.dot(onehot.astype(bf16), before, preferred_element_type=f32) + base
        rank = jnp.sum(earlier * onehot, axis=0, keepdims=True).astype(jnp.int32)
        base = base + jnp.sum(onehot, axis=1, keepdims=True)
        where = slot_of(label, rank, capacity, direct)
        slots_out[j : j + 1, :] = where
        if direct:
            there = slot_of(label, rank, capacity, direct, 1)
            own_far = jnp.logical_and(there >= 2 * capacity, there < 3 * capacity)
            there = jnp.where(own_far, there + 2 * capacity, -1)
            slots_out[j : j + 1, :] = jnp.maximum(where, there)
        hit = jnp.where(slot == where, 1.0, hit)
    pick = hit.astype(bf16)
    copies[1].wait()
    copies[2].wait()
    values = tokens[...].astype(f32)
    scale = lax.rsqrt(jnp.mean(values * values, axis=-1, keepdims=True) + norm_eps)
    lanes = gain.shape[1]
    for c in range(width // lanes):
        at = slice(c * lanes, (c + 1) * lanes)
        normed_out[:, at] = (values[:, at] * scale * gain[c : c + 1].astype(f32)).astype(bf16)
    rest, far = outs[2], outs[3:]
    n = rest.shape[0]
    rest[...] = pick[:n]
    for out in far:
        out[...] = jnp.dot(pick[n:], normed_out[...], preferred_element_type=f32).astype(bf16)


def spread_body(pick, normed, *refs):
    sources, copied, outs, sems = refs[:3], refs[3:6], refs[6:-1], refs[-1]
    copies = fetch(sources, copied, sems)
    at = 0
    for out in outs:
        n = out.shape[0]
        part = pick[at : at + n]
        out[...] = jnp.dot(part, normed[...], preferred_element_type=f32).astype(bf16)
        at += n
    for copy in copies:
        copy.wait()


def units_of(rows, weights):
    into = [w[...] for w in weights[::3]] + [w[...] for w in weights[1::3]]
    both = jnp.dot(rows, jnp.concatenate(into, axis=1), preferred_element_type=f32)
    units = both.shape[1] // 2
    gate, up = both[:, :units], both[:, units:]
    return (gate / (1.0 + jnp.exp(-gate)) * up).astype(bf16)


def shared_body(groups, total, slots, rows, *refs):
    weights, gains_in, part, outs = refs[:3], refs[3], refs[4], refs[5:-2]
    gains, sems = refs[-2:]
    (copy,) = fetch((gains_in,), (gains,), sems)
    hidden = units_of(rows[...], weights)
    part[...] = jnp.dot(hidden, weights[2][...], preferred_element_type=f32)
    slot = lax.broadcasted_iota(jnp.int32, (total, rows.shape[0]), 0)
    weight = jnp.zeros(slot.shape, f32)
    copy.wait()
    for j in range(slots.shape[0]):
        weight = jnp.where(slot == slots[j : j + 1, :], gains[j : j + 1, :], weight)
    high = weight.astype(bf16).astype(f32)
    low = weight - high
    for out, spans in zip(outs, groups):
        parts = [half[a:b] for a, b in spans for half in (high, low)]
        out[...] = jnp.concatenate(parts, axis=0).T.astype(bf16)


def near_body(blocks, *refs):
    rows_in, weights = refs[:blocks], refs[blocks : blocks + 6]
    outs = refs[blocks + 6 : 2 * blocks + 6]
    gathered = gather_rows(rows_in, refs[-1])
    down = jnp.concatenate([w[...] for w in weights[2::3]], axis=0)
    hidden = units_of(gathered[...], weights)
    total = jnp.dot(hidden, down, preferred_element_type=f32).astype(bf16)
    at = 0
    for out in outs:
        out[...] = total[at : at + out.shape[0]]
        at += out.shape[0]


def gather_rows(rows_in, room):
    if len(rows_in) == 1:
        return rows_in[0]
    at = 0
    for ref in rows_in:
        room[at : at + ref.shape[0]] = ref[...]
        at += ref.shape[0]
    return room


def picked(weights, rows):
    return jnp.dot(weights[...], rows, preferred_element_type=f32)


def first_body(blocks, weights, part, *refs):
    rows_in, (send, keep) = refs[:blocks], refs[blocks : blocks + 2]
    gathered = gather_rows((*rows_in, *rows_in), refs[-1])
    share = keep.shape[1] // 2
    core = lax.axis_index("tp") % 2
    for out, place in ((send, 1 - core), (keep, core)):
        for x in range(2):
            columns = pl.ds(pl.multiple_of((2 * x + place) * share, share), share)
            total = part[:, columns] + picked(weights, gathered[:, columns])
            out[:, x * share : (x + 1) * share] = total.astype(out.dtype)


def halve_body(keep, came, send, mine):
    share = mine.shape[1]
    side = lax.axis_index("tp") // 2
    for out, place in ((send, 1 - side), (mine, side)):
        columns = pl.ds(pl.multiple_of(place * share, share), share)
        out[...] = (keep[:, columns] + came[:, columns].astype(f32)).astype(out.dtype)


def columns_out(hidden, weights, send, keep):
    side = lax.axis_index("tp") // 2
    width = keep.shape[1]
    for out, place in ((send, 1 - side), (keep, side)):
        columns = pl.ds(pl.multiple_of(place * width, width), width)
        down = jnp.concatenate([w[:, columns] for w in weights[2::3]], axis=0)
        out[...] = jnp.dot(hidden, down, preferred_element_type=f32).astype(out.dtype)


def product_body(*refs):
    rows, weights, send, keep = refs[0], refs[1:7], refs[7], refs[8]
    columns_out(units_of(rows[...], weights), weights, send, keep)


def products(body, rows, weights, outs):
    n = sum(r.shape[0] for r in rows)
    full = rows[0].shape[1]
    hidden = sum(w.shape[1] for w in weights[::3])
    scratch = [pltpu.VMEM((n, full), bf16)] if len(rows) > 1 else []
    return call(body, outs, [*rows, *weights], 6 * n * full * hidden, scratch)


def add_body(keep, came, *outs):
    if len(outs) == 1:
        outs[0][...] = (keep[...] + came[...].astype(f32)).astype(outs[0].dtype)
        return
    width = outs[0].shape[1]
    core = lax.axis_index("tp") % 2
    for out, place in ((outs[0], core), (outs[1], 1 - core)):
        columns = pl.ds(pl.multiple_of(place * width, width), width)
        out[...] = (keep[:, columns] + came[:, columns].astype(f32)).astype(out.dtype)


def swap_body(weights, rows, mine, send, keep, room):
    gathered = gather_rows((rows, rows), room)
    width = keep.shape[1]
    core = lax.axis_index("tp") % 2
    columns = pl.ds(pl.multiple_of((1 - core) * width, width), width)
    send[...] = picked(weights, gathered[:, columns])
    columns = pl.ds(pl.multiple_of(core * width, width), width)
    keep[...] = picked(weights, gathered[:, columns]) + mine[...]


def mix_body(weights, rows, rows2, came, kept, swapped, out, room):
    gathered = gather_rows((rows, rows, rows2, rows2), room)
    total = came[...].astype(f32) + kept[...] + swapped[...]
    out[...] = (total + picked(weights, gathered[...])).astype(out.dtype)


def local(
    tokens,
    norm_gain,
    expert_ids,
    route_weights,
    gate_weight,
    up_weight,
    down_weight,
    shared_gate,
    shared_up,
    shared_down,
):
    rows_here, width = tokens.shape
    chosen = expert_ids.shape[1]
    groups = lax.axis_size("ep")
    cuts = lax.axis_size("tp")
    local_experts = gate_weight.shape[0]
    assert local_experts == 1 and cuts == 4
    capacity = (3 * rows_here * chosen + 2 * groups - 1) // (2 * groups)
    wide, share = width // 2, width // 4
    direct = groups == 8
    sibling = [(i, i ^ 1) for i in range(cuts)]
    neighbour = [(i, i ^ 2) for i in range(cuts)]
    own = (gate_weight[0], up_weight[0], down_weight[0])
    other = tuple(lax.ppermute(w, "tp", sibling) for w in own)

    def hop(block, between, flip=0):
        if not direct:
            return lax.all_to_all(block, "ep", split_axis=0, concat_axis=0, tiled=True)
        pairs = []
        for i in range(groups):
            for t in range(cuts):
                to = i ^ between(t // 2, t % 2)
                pairs.append((i * cuts + t, to * cuts + (t ^ flip)))
        return lax.ppermute(block, ("ep", "tp"), pairs)

    distances = {
        "P": lambda x, c: c,
        "Q": lambda x, c: 3 - c,
        "A": lambda x, c: (4 + 3 * c) ^ x,
        "B": lambda x, c: (4 + 3 * c) ^ x ^ 1,
    }
    half = -(-capacity // 2)
    sizes = {k: capacity for k in distances} if direct else {"P": half * groups}
    sent_here = [k for k in sizes if k != "B"]
    total = sum(sizes.values())
    args = [expert_ids.T, norm_gain.reshape(-1, 128), tokens]
    sh_weights = [shared_gate, shared_up, shared_down]
    ahead = ["A"] if direct else []
    later = [k for k in sent_here if k not in ahead]
    n_later = sum(sizes[k] for k in later)
    normed, slots, pick, *sends = call(
        functools.partial(route_body, capacity, groups, direct),
        [shape(rows_here, width, bf16), shape(chosen, rows_here, jnp.int32)]
        + [shape(n_later, rows_here, bf16)]
        + [shape(sizes[k], width, bf16) for k in ahead],
        args,
        2 * rows_here * width * total,
        landing(args),
        range(3),
    )
    rest = call(
        spread_body,
        [shape(*w.shape, w.dtype) for w in sh_weights]
        + [shape(sizes[k], width, bf16) for k in later],
        [pick, normed, *sh_weights],
        2 * rows_here * width * n_later,
        [pltpu.SemaphoreType.DMA((3,))],
        range(2, 5),
    )
    sh_weights, sends = rest[:3], [*rest[3:], *sends]
    arrived = {k: hop(block, distances[k]) for k, block in zip(sent_here, sends)}
    if direct:
        arrived["B"] = lax.ppermute(arrived["A"], "tp", neighbour)
    near = [k for k in sizes if k in ("P", "Q")]
    n_near = sum(sizes[k] for k in near)
    groups_of = [[(0, n_near)]]
    if direct:
        at = [i * capacity for i in range(6)]
        groups_of += [[(at[3], at[4])], [(at[2], at[3]), (at[4], at[5])]]
        total = at[5]
    gains = route_weights.T
    part, *weights = call(
        functools.partial(shared_body, groups_of, total),
        [shape(rows_here, width, f32)]
        + [shape(rows_here, 2 * sum(b - a for a, b in spans), bf16) for spans in groups_of],
        [slots, normed, *sh_weights, gains],
        6 * rows_here * width * shared_gate.shape[1],
        landing([gains]),
        [5],
    )

    outs = [shape(sizes[k], width, bf16) for k in near]
    body = functools.partial(near_body, len(near))
    outs = products(body, [arrived[k] for k in near], [*own, *other], outs)
    returned = {k: hop(out, distances[k]) for k, out in zip(near, outs)}
    send, keep = call(
        functools.partial(first_body, len(near)),
        [shape(rows_here, wide, bf16), shape(rows_here, wide, f32)],
        [weights[0], part, *[returned[k] for k in near]],
        4 * rows_here * width * n_near,
        [pltpu.VMEM((2 * n_near, width), bf16)],
    )
    send, mine = call(
        halve_body,
        [shape(rows_here, share, bf16), shape(rows_here, share, f32)],
        [keep, lax.ppermute(send, "tp", sibling)],
        keep.size,
    )
    came = lax.ppermute(send, "tp", neighbour)

    if direct:
        sent, kept = {}, {}
        for k in "AB":
            outs = [shape(capacity, wide, bf16), shape(capacity, wide, f32)]
            sent[k], kept[k] = products(product_body, [arrived[k]], [*own, *other], outs)
            sent[k] = lax.ppermute(sent[k], "tp", neighbour)
        ins, outs = [kept["B"], sent["A"]], [shape(capacity, wide, bf16)]
        (out,) = call(add_body, outs, ins, kept["B"].size)
        out = hop(out, distances["B"])
        send, swap_mine = call(
            swap_body,
            [shape(rows_here, share, f32)] * 2,
            [weights[1], out, mine],
            4 * rows_here * wide * capacity,
            [pltpu.VMEM((2 * capacity, wide), bf16)],
        )
        swap_came = lax.ppermute(send, "tp", sibling)
        ins, outs = [kept["A"], sent["B"]], [shape(capacity, share, bf16)] * 2
        outs = call(add_body, outs, ins, kept["A"].size)
        rows = [hop(out, distances["A"], flip) for flip, out in enumerate(outs)]
        (mixed,) = call(
            mix_body,
            [shape(rows_here, share, bf16)],
            [weights[2], *rows, came, swap_mine, swap_came],
            8 * rows_here * share * capacity,
            [pltpu.VMEM((4 * capacity, share), bf16)],
        )
        return mixed
    (mixed,) = call(add_body, [shape(rows_here, share, bf16)], [mine, came], mine.size)
    return mixed


def solution(mesh):
    in_specs = (
        P("ep", None),
        P(),
        P("ep", None),
        P("ep", None),
        P("ep", None, "tp"),
        P("ep", None, "tp"),
        P("ep", "tp", None),
        P(None, "tp"),
        P(None, "tp"),
        P("tp", None),
    )
    out_specs = P("ep", "tp")

    return jax.shard_map(local, mesh=mesh, in_specs=in_specs, out_specs=out_specs, check_vma=False)
```
